128 devices in a mesh: kv: 16 (over z, x), tp: 8 (over y, core).
Axes of the slice: x: 4, y: 4, z: 4, core: 2. Of those that a mesh axis runs over, the one named last changes fastest.
Arguments:
- tokens: bfloat16 [32768, 2048], P('kv'), may hold values from -6 to 6
- norm_gain: bfloat16 [2048], replicated, may hold values from 0.099609375 to 1.8984375
- query_weight: bfloat16 [2048, 1024], P(None, 'tp'), may hold values from -0.125 to 0.125
- cmp_key_weight: bfloat16 [2048, 512], P(None, 'tp'), may hold values from -0.125 to 0.125
- cmp_value_weight: bfloat16 [2048, 512], P(None, 'tp'), may hold values from -0.125 to 0.125
- sel_key_weight: bfloat16 [2048, 512], P(None, 'tp'), may hold values from -0.125 to 0.125
- sel_value_weight: bfloat16 [2048, 512], P(None, 'tp'), may hold values from -0.125 to 0.125
- branch_weight: bfloat16 [2, 2048, 16], replicated, may hold values from -0.125 to 0.125
- key_embed: bfloat16 [8, 32, 64], P('tp'), may hold values from -3 to 3
- key_inner: bfloat16 [8, 2048, 64], P('tp'), may hold values from -0.125 to 0.125
- key_outer: bfloat16 [8, 64, 64], P('tp'), may hold values from -0.75 to 0.75
- value_embed: bfloat16 [8, 32, 64], P('tp'), may hold values from -3 to 3
- value_inner: bfloat16 [8, 2048, 64], P('tp'), may hold values from -0.125 to 0.125
- value_outer: bfloat16 [8, 64, 64], P('tp'), may hold values from -0.75 to 0.75
- out_weight: bfloat16 [1024, 2048], replicated, may hold values from -0.1875 to 0.1875
- chosen: int32 [8, 256, 8], P('tp'), may hold values from 0 to 511, as said below
Outputs:
- attended: bfloat16 [32768, 2048], P(('kv', 'tp'))
The draws below stay inside these ranges and needn't reach their ends.
Inputs may be any that keep to these rules, and one draw needn't show every extreme that they name: `chosen`: each entry is the index of a block of 64 positions in the whole sequence. For every key head and query block, its 8 entries lie in 8 different aligned spans of 2048 positions (at most one from any span), and none lies inside the query block's own positions.
All inputs are finite; a program needn't handle non-finite values.
Results may differ from the reference program's by a relative error of at most 0.0075.
Values may be sent and summed in bfloat16 or wider, within the bound.
No kernel may reach another device: no remote copies, remote signals or barrier semaphores. Data moves between devices by JAX's collectives and lax.ppermute only.
A program may use at most 128 MiB of HBM per device.

```python
import jax
import jax.numpy as jnp
from jax import lax

D = 2048
HEADS = 16
KV_HEADS = 8
HEAD_DIM = 64
CMP_BLOCK = 32
SEL_BLOCK = 64
Q_BLOCK = 128
FAR_PICKS = 8
TOK_DEV = 2048
SEQ = 32768


def draw_chosen(key, part):
    interval_limits = SEQ // TOK_DEV
    per_span = TOK_DEV // Q_BLOCK
    span_blocks = TOK_DEV // SEL_BLOCK
    own_blocks = Q_BLOCK // SEL_BLOCK
    query_blocks = SEQ // Q_BLOCK
    key_noise, key_inner, key_shift = jax.random.split(key, 3)
    diagonal_group = jnp.arange(query_blocks, dtype=jnp.int32) // per_span
    local_index = jnp.arange(query_blocks, dtype=jnp.int32) % per_span
    eligible_group = jnp.arange(interval_limits, dtype=jnp.int32)
    jitter_perturbation = jax.random.randint(key_noise, (KV_HEADS, query_blocks, interval_limits), 0, 2 ** 16)
    preference_increment = jnp.where(eligible_group[None, :] <= diagonal_group[:, None], 2 ** 24, 0)
    preference_increment = preference_increment + jnp.where(eligible_group[None, :] == diagonal_group[:, None] - 1, 2 ** 26, 0)
    preference_increment = preference_increment + jnp.where(eligible_group[None, :] == diagonal_group[:, None] - interval_limits // 2, 2 ** 26, 0)
    preference_increment = preference_increment + jnp.where(eligible_group[None, :] == 0, 2 ** 25, 0)
    group_relevance = jitter_perturbation * interval_limits + eligible_group[None, None, :] + preference_increment[None]
    _, picked = lax.top_k(group_relevance, FAR_PICKS)
    inside = jax.random.randint(key_inner, (KV_HEADS, query_blocks, FAR_PICKS), 0, span_blocks)
    offset = jax.random.randint(key_shift, (KV_HEADS, query_blocks, FAR_PICKS), 0, span_blocks - own_blocks)
    shifted = (local_index[None, :, None] * own_blocks + own_blocks + offset) % span_blocks
    within = jnp.where(picked == diagonal_group[None, :, None], shifted, inside)
    return (picked * span_blocks + within).astype(jnp.int32)


def block_scale(rng, dims, pieces, smallest, top_value):
    def one(axis_at, blocks):
        draws = jax.random.uniform(jax.random.fold_in(jax.random.fold_in(rng, 6), axis_at), (blocks,), jnp.float32, smallest / len(pieces), top_value / len(pieces))
        return jnp.repeat(jnp.exp(draws), dims[axis_at] // blocks).reshape((-1,) + (1,) * (len(dims) - axis_at - 1))

    factor_of = one(*pieces[0])
    for cut in pieces[1:]:
        factor_of = factor_of * one(*cut)
    return factor_of


def bell_draw(own_key, shape, scale, bound, cuts=(), kind=jnp.bfloat16):
    level = block_scale(own_key, shape, cuts, -0.22, 0.18) if cuts else 1.0
    result = jax.random.normal(own_key, shape, jnp.float32) * scale * level
    return jnp.minimum(jnp.maximum(result, -bound), bound).astype(kind)


def setup_inputs(seed: int = 0) -> dict:
    splits = jax.random.split(jax.random.key(seed), 17)
    return {
        "tokens": bell_draw(splits[0], (SEQ, D), 1.0, 6.0, ((0, 16),)),
        "norm_gain": jnp.clip(1.0 + 0.18 * jax.random.normal(splits[1], (D,), jnp.float32), 0.099609375, 1.8984375).astype(jnp.bfloat16),
        "query_weight": bell_draw(splits[2], (D, HEADS * HEAD_DIM), D ** -0.5, 0.125, ((1, 8),)),
        "cmp_key_weight": bell_draw(splits[3], (D, KV_HEADS * HEAD_DIM), D ** -0.5, 0.125, ((1, 8),)),
        "cmp_value_weight": bell_draw(splits[4], (D, KV_HEADS * HEAD_DIM), D ** -0.5, 0.125, ((1, 8),)),
        "sel_key_weight": bell_draw(splits[5], (D, KV_HEADS * HEAD_DIM), D ** -0.5, 0.125, ((1, 8),)),
        "sel_value_weight": bell_draw(splits[6], (D, KV_HEADS * HEAD_DIM), D ** -0.5, 0.125, ((1, 8),)),
        "branch_weight": bell_draw(splits[7], (2, D, HEADS), D ** -0.5, 0.125),
        "key_embed": bell_draw(splits[8], (KV_HEADS, CMP_BLOCK, HEAD_DIM), 0.5, 3.0, ((0, 8),)),
        "key_inner": bell_draw(splits[9], (KV_HEADS, CMP_BLOCK * HEAD_DIM, HEAD_DIM), (CMP_BLOCK * HEAD_DIM) ** -0.5, 0.125, ((0, 8),)),
        "key_outer": bell_draw(splits[10], (KV_HEADS, HEAD_DIM, HEAD_DIM), HEAD_DIM ** -0.5, 0.75, ((0, 8),)),
        "value_embed": bell_draw(splits[11], (KV_HEADS, CMP_BLOCK, HEAD_DIM), 0.5, 3.0, ((0, 8),)),
        "value_inner": bell_draw(splits[12], (KV_HEADS, CMP_BLOCK * HEAD_DIM, HEAD_DIM), (CMP_BLOCK * HEAD_DIM) ** -0.5, 0.125, ((0, 8),)),
        "value_outer": bell_draw(splits[13], (KV_HEADS, HEAD_DIM, HEAD_DIM), HEAD_DIM ** -0.5, 0.75, ((0, 8),)),
        "out_weight": bell_draw(splits[14], (HEADS * HEAD_DIM, D), (HEADS * HEAD_DIM) ** -0.5, 0.1875),
        "chosen": draw_chosen(jax.random.fold_in(splits[16], 71), 0),
    }


ROPE_BASE = 10000.0
norm_eps = 1e-06
masked_score = -1000000000.0

def rotate(values_in, positions):
    half_dim = values_in.shape[-1] // 2
    inverse = ROPE_BASE ** (-jnp.arange(half_dim, dtype=jnp.float32) / half_dim)
    rotary_phases = positions.astype(jnp.float32)[:, None] * inverse[None, :]
    cosine = jnp.cos(rotary_phases)[:, None, :]
    sine = jnp.sin(rotary_phases)[:, None, :]
    first_half = values_in[..., :half_dim]
    second_half = values_in[..., half_dim:]
    return jnp.concatenate([first_half * cosine - second_half * sine, second_half * cosine + first_half * sine], axis=-1)

def summarize(raw_rows, embed, inner, outer):
    block_count = raw_rows.shape[0] // CMP_BLOCK
    blocked = raw_rows.reshape(block_count, CMP_BLOCK, KV_HEADS, HEAD_DIM).transpose(2, 0, 1, 3).astype(jnp.float32)
    blocked = (blocked + embed.astype(jnp.float32)[:, None]).astype(jnp.bfloat16)
    blocked = blocked.reshape(KV_HEADS, block_count, CMP_BLOCK * HEAD_DIM)
    hidden = jax.nn.gelu(jnp.einsum('knc,kce->kne', blocked.astype(jnp.float32), inner.astype(jnp.float32))).astype(jnp.bfloat16)
    return jnp.einsum('kne,kef->knf', hidden.astype(jnp.float32), outer.astype(jnp.float32)).astype(jnp.bfloat16)

def reference(tokens, norm_gain, query_weight, cmp_key_weight, cmp_value_weight, sel_key_weight, sel_value_weight, branch_weight, key_embed, key_inner, key_outer, value_embed, value_inner, value_outer, out_weight, chosen):
    length = tokens.shape[0]
    group_size = HEADS // KV_HEADS
    positions = jnp.arange(length, dtype=jnp.int32)
    scale = HEAD_DIM ** (-0.5)
    expanded_mask = tokens.astype(jnp.float32)
    normed = (expanded_mask * lax.rsqrt(lax.optimization_barrier(jnp.mean(expanded_mask * expanded_mask, axis=-1, keepdims=True)) + norm_eps) * norm_gain.astype(jnp.float32)).astype(jnp.bfloat16)

    def project(weight_in):
        return jnp.dot(normed, weight_in, preferred_element_type=jnp.float32)
    query = project(query_weight).reshape(length, HEADS, HEAD_DIM)
    q_plain = query.astype(jnp.bfloat16)
    q_turn = rotate(query, positions).astype(jnp.bfloat16)
    cmp_key = project(cmp_key_weight).astype(jnp.bfloat16).reshape(length, KV_HEADS, HEAD_DIM)
    cmp_value = project(cmp_value_weight).astype(jnp.bfloat16).reshape(length, KV_HEADS, HEAD_DIM)
    sel_key = rotate(project(sel_key_weight).reshape(length, KV_HEADS, HEAD_DIM), positions).astype(jnp.bfloat16)
    selected_value = project(sel_value_weight).astype(jnp.bfloat16).reshape(length, KV_HEADS, HEAD_DIM)
    gate_cmp = jax.nn.sigmoid(project(branch_weight[0]))
    gate_sel = jax.nn.sigmoid(project(branch_weight[1]))
    summary_key = summarize(cmp_key, key_embed, key_inner, key_outer)
    summary_value = summarize(cmp_value, value_embed, value_inner, value_outer)
    summary_count = summary_key.shape[1]
    block_end = (jnp.arange(summary_count, dtype=jnp.int32) + 1) * CMP_BLOCK - 1

    def compress_head(packed_rows):
        head_query, head_keys, head_values = packed_rows
        scores = jnp.einsum('tgd,cd->tgc', head_query.astype(jnp.float32), head_keys.astype(jnp.float32)) * scale
        allowed_keys = (block_end[None, :] <= positions[:, None])[:, None, :]
        probs = jax.nn.softmax(jnp.where(allowed_keys, scores, masked_score), axis=-1) * allowed_keys.astype(jnp.float32)
        return jnp.einsum('tgc,cd->tgd', probs.astype(jnp.bfloat16).astype(jnp.float32), head_values.astype(jnp.float32))
    q_group = q_plain.reshape(length, KV_HEADS, group_size, HEAD_DIM).transpose(1, 0, 2, 3)
    out_cmp = lax.map(compress_head, (q_group, summary_key, summary_value))
    out_cmp = out_cmp.transpose(1, 0, 2, 3).reshape(length, HEADS, HEAD_DIM)
    query_blocks = length // Q_BLOCK
    block_pos = jnp.arange(query_blocks, dtype=jnp.int32)[:, None] * Q_BLOCK + jnp.arange(Q_BLOCK, dtype=jnp.int32)[None, :]

    def select_head(packed_rows):
        head_query, head_keys, head_values, head_picks = packed_rows
        far_keys = head_keys.reshape(-1, SEL_BLOCK, HEAD_DIM)[head_picks].reshape(query_blocks, FAR_PICKS * SEL_BLOCK, HEAD_DIM)
        far_values = head_values.reshape(-1, SEL_BLOCK, HEAD_DIM)[head_picks].reshape(query_blocks, FAR_PICKS * SEL_BLOCK, HEAD_DIM)
        all_keys = jnp.concatenate([head_keys.reshape(query_blocks, Q_BLOCK, HEAD_DIM), far_keys], axis=1)
        all_values = jnp.concatenate([head_values.reshape(query_blocks, Q_BLOCK, HEAD_DIM), far_values], axis=1)
        far_pos = (head_picks[:, :, None] * SEL_BLOCK + jnp.arange(SEL_BLOCK, dtype=jnp.int32)[None, None, :]).reshape(query_blocks, -1)
        key_pos = jnp.concatenate([block_pos, far_pos], axis=1)
        allowed_keys = key_pos[:, None, None, :] <= block_pos[:, :, None, None]
        scores = jnp.einsum('nqgd,nmd->nqgm', head_query.astype(jnp.float32), all_keys.astype(jnp.float32)) * scale
        probs = jax.nn.softmax(jnp.where(allowed_keys, scores, masked_score), axis=-1)
        return jnp.einsum('nqgm,nmd->nqgd', probs.astype(jnp.bfloat16).astype(jnp.float32), all_values.astype(jnp.float32))
    q_sel = q_turn.reshape(query_blocks, Q_BLOCK, KV_HEADS, group_size, HEAD_DIM).transpose(2, 0, 1, 3, 4)
    out_sel = lax.map(select_head, (q_sel, sel_key.transpose(1, 0, 2), selected_value.transpose(1, 0, 2), chosen.astype(jnp.int32)))
    out_sel = out_sel.transpose(1, 2, 0, 3, 4).reshape(length, HEADS, HEAD_DIM)
    mixed = (gate_cmp[..., None] * out_cmp + gate_sel[..., None] * out_sel).reshape(length, HEADS * HEAD_DIM).astype(jnp.bfloat16)
    return jnp.dot(mixed, out_weight, preferred_element_type=jnp.float32).astype(jnp.bfloat16)
```

```python
import functools

import jax
import jax.numpy as jnp
import numpy as np
from jax import lax
from jax.experimental import pallas as pl
from jax.experimental.pallas import tpu as pltpu
from jax.sharding import PartitionSpec as P

HEAD_DIM = 64
CMP_BLOCK = 32
SEL_BLOCK = 64
Q_BLOCK = 128
FAR_PICKS = 8
ROPE_BASE = 10000.0
NORM_EPS = 1e-06
MASKED = -1e30
LANES = 128
TILE = 256

F32 = jnp.float32
BF16 = jnp.bfloat16


def dot_nt(a, b):
    return lax.dot_general(a, b, (((1,), (1,)), ((), ())), preferred_element_type=F32)


def rope_tables(total):
    lane = np.arange(LANES)
    inverse = ROPE_BASE ** (-(lane % 32) / 32.0)
    sign = np.where(lane % 64 < 32, -1.0, 1.0)
    coarse = (np.arange(total // TILE) * TILE)[:, None] * inverse[None, :]
    fine = np.arange(TILE)[:, None] * inverse[None, :]
    pack = lambda a: np.stack([np.cos(a), np.sin(a) * sign[None, :]], axis=1).astype(np.float32)
    return pack(coarse), pack(fine).transpose(1, 0, 2)


def project_kernel(
    meta, tok_ref, gain_ref, wq_ref, sk_ref, sv_ref, ck_ref, cv_ref, bw_ref, coarse_ref, fine_ref,
    ke_ref, ki_ref, ko_ref, ve_ref, vi_ref, vo_ref,
    qp_ref, qt_ref, kv_ref, gc_ref, gs_ref, first_ref, second_ref,
    w_scr, kv_scr, c_scr,
):
    step = pl.program_id(0)
    lane = lax.broadcasted_iota(jnp.int32, (TILE, LANES), 1)
    low = lane < HEAD_DIM

    @pl.when(step == 0)
    def _():
        w_scr[:, 0:LANES] = wq_ref[...]
        w_scr[:, LANES:2 * LANES] = jnp.concatenate([sk_ref[...], sv_ref[...]], axis=0).T
        w_scr[:, 2 * LANES:3 * LANES] = jnp.concatenate([ck_ref[...], cv_ref[...]], axis=0).T
        bw = bw_ref[...]
        pad = jnp.zeros((LANES - bw.shape[0], bw.shape[1]), BF16)
        w_scr[:, 3 * LANES:4 * LANES] = jnp.concatenate([bw, pad], axis=0).T

    x = tok_ref[...].astype(F32)
    mean = jnp.mean(x * x, axis=-1, keepdims=True)
    normed = (x * lax.rsqrt(mean + NORM_EPS) * gain_ref[...].astype(F32)).astype(BF16)
    proj = jnp.dot(normed, w_scr[...], preferred_element_type=F32)

    ch = coarse_ref[0, 0:1, :]
    sh = coarse_ref[0, 1:2, :]
    cl = fine_ref[0]
    sl = fine_ref[1]
    cosine = ch * cl - sh * sl
    sine = sh * cl + ch * sl
    first_half = (lane % HEAD_DIM) < 32

    def turn(v):
        swapped = jnp.where(first_half, pltpu.roll(v, LANES - 32, 1), pltpu.roll(v, 32, 1))
        return v * cosine + swapped * sine

    q = proj[:, 0:LANES]
    scale = HEAD_DIM ** (-0.5)
    plain = q * scale
    turned = turn(q) * scale
    qp_ref[0] = jnp.where(low, plain, 0.0).astype(BF16)
    qp_ref[1] = jnp.where(low, pltpu.roll(plain, HEAD_DIM, 1), 0.0).astype(BF16)
    qt_ref[0] = jnp.where(low, turned, 0.0).astype(BF16)
    qt_ref[1] = jnp.where(low, pltpu.roll(turned, HEAD_DIM, 1), 0.0).astype(BF16)
    kv = proj[:, LANES:2 * LANES]
    kv = jnp.where(low, turn(kv), kv).astype(BF16)
    kv_ref[...] = kv
    per = TILE // SEL_BLOCK
    kv_scr[pl.ds(step * per, per)] = kv.reshape(per, SEL_BLOCK, LANES)
    rows = pl.multiple_of(step * TILE, TILE)
    c_scr[pl.ds(rows, TILE), :] = proj[:, 2 * LANES:3 * LANES].astype(BF16).astype(F32)
    heads = meta[meta.shape[0] - 1] * 2
    logits = pltpu.roll(proj[:, 3 * LANES:4 * LANES], LANES - heads, 1)
    gates = 1.0 / (1.0 + jnp.exp(-logits))
    gc_ref[...] = jnp.where(low, gates[:, 0:1], gates[:, 1:2])
    gs_ref[...] = jnp.where(low, gates[:, 16:17], gates[:, 17:18])

    @pl.when(step == pl.num_programs(0) - 1)
    def _():
        blocks = first_ref.shape[2]
        low_b = lax.broadcasted_iota(jnp.int32, (blocks, LANES), 1) < HEAD_DIM
        key_parts = []
        value_parts = []
        for pair in range(CMP_BLOCK // 2):
            two = []
            for r in (2 * pair, 2 * pair + 1):
                embed = jnp.concatenate([ke_ref[r:r + 1, :], ve_ref[r:r + 1, :]], axis=1).astype(F32)
                two.append(c_scr[pl.ds(r, blocks, stride=CMP_BLOCK), :] + embed)
            a, b = two
            key_parts.append(jnp.where(low_b, a, pltpu.roll(b, HEAD_DIM, 1)).astype(BF16))
            value_parts.append(jnp.where(low_b, pltpu.roll(a, HEAD_DIM, 1), b).astype(BF16))
        hidden_k = jax.nn.gelu(dot_nt(jnp.concatenate(key_parts, axis=1), ki_ref[...])).astype(BF16)
        hidden_v = jax.nn.gelu(dot_nt(jnp.concatenate(value_parts, axis=1), vi_ref[...])).astype(BF16)
        summary = jnp.concatenate(
            [
                jnp.dot(hidden_k, ko_ref[...], preferred_element_type=F32),
                jnp.dot(hidden_v, vo_ref[...], preferred_element_type=F32),
            ],
            axis=1,
        ).astype(BF16)
        owners = first_ref.shape[0]
        half = second_ref.shape[1]

        def fill(d, carry):
            for j in range(half):
                first_ref[d, j] = kv_scr[meta[d * 2 * half + 2 * j]]
                second_ref[d, j] = kv_scr[meta[d * 2 * half + 2 * j + 1]]
            first_ref[d, half] = summary
            return carry

        lax.fori_loop(0, owners, fill, 0)


def compress_kernel(meta, qp_ref, sum_ref, gc_ref, out_ref, v_scr):
    step = pl.program_id(0)
    owners, _, blocks, _ = sum_ref.shape
    count = owners * blocks

    @pl.when(step == 0)
    def _():
        low_k = lax.broadcasted_iota(jnp.int32, (count, LANES), 1) < HEAD_DIM
        v_scr[...] = jnp.where(low_k, 1.0, sum_ref[...].reshape(count, LANES).astype(F32)).astype(BF16)

    keys = sum_ref[...].reshape(count, LANES)
    q = qp_ref[...].reshape(2 * Q_BLOCK, LANES)
    scores = dot_nt(q, keys)
    base = meta[0] + step * Q_BLOCK
    row = lax.broadcasted_iota(jnp.int32, (2 * Q_BLOCK, 1), 0) % Q_BLOCK
    limit = (base + row + 1) // CMP_BLOCK
    col = lax.broadcasted_iota(jnp.int32, (2 * Q_BLOCK, count), 1)
    scores = jnp.where(col < limit, scores, MASKED)
    top = jnp.max(scores, axis=-1, keepdims=True)
    probs = jnp.exp(scores - top).astype(BF16)
    mixed = jnp.dot(probs, v_scr[...], preferred_element_type=F32)
    total = pltpu.roll(mixed, HEAD_DIM, 1)
    out = jnp.where(limit > 0, mixed / total, 0.0)
    low = lax.broadcasted_iota(jnp.int32, (Q_BLOCK, LANES), 1) < HEAD_DIM
    joined = jnp.where(low, pltpu.roll(out[:Q_BLOCK], HEAD_DIM, 1), out[Q_BLOCK:])
    out_ref[...] = gc_ref[...] * joined


def select_kernel(src, qt_ref, kv_ref, in_ref, bias_ref, gs_ref, cmp_ref, out_ref, k_scr, v_scr, *, parity):
    step = pl.program_id(0)
    k_scr[0:Q_BLOCK, :] = kv_ref[...]
    block = 2 * step + parity
    for j in range(FAR_PICKS):
        k_scr[Q_BLOCK + j * SEL_BLOCK:Q_BLOCK + (j + 1) * SEL_BLOCK, :] = in_ref[src[block * FAR_PICKS + j], 0]
    keys = k_scr[...]
    total_keys = keys.shape[0]
    low_k = lax.broadcasted_iota(jnp.int32, (total_keys, LANES), 1) < HEAD_DIM
    v_scr[...] = jnp.where(low_k, 1.0, keys.astype(F32)).astype(BF16)
    q = qt_ref[...].reshape(2 * Q_BLOCK, LANES)
    scores = dot_nt(q, keys)
    row = lax.broadcasted_iota(jnp.int32, (2 * Q_BLOCK, Q_BLOCK), 0) % Q_BLOCK
    col = lax.broadcasted_iota(jnp.int32, (2 * Q_BLOCK, Q_BLOCK), 1)
    own = jnp.where(col <= row, scores[:, :Q_BLOCK], MASKED)
    far = scores[:, Q_BLOCK:] + bias_ref[0]
    top = jnp.maximum(jnp.max(own, axis=-1, keepdims=True), jnp.max(far, axis=-1, keepdims=True))
    probs_own = jnp.exp(own - top).astype(BF16)
    probs_far = jnp.exp(far - top).astype(BF16)
    mixed = jnp.dot(jnp.concatenate([probs_own, probs_far], axis=1), v_scr[...], preferred_element_type=F32)
    out = mixed / pltpu.roll(mixed, HEAD_DIM, 1)
    low = lax.broadcasted_iota(jnp.int32, (Q_BLOCK, LANES), 1) < HEAD_DIM
    joined = jnp.where(low, pltpu.roll(out[:Q_BLOCK], HEAD_DIM, 1), out[Q_BLOCK:])
    out_ref[0] = (cmp_ref[...] + gs_ref[...] * joined).astype(BF16)


def whole(shape):
    return pl.BlockSpec(shape, lambda i, *_: (0,) * len(shape))


def per_device(
    tokens, norm_gain, query_weight, cmp_key_weight, cmp_value_weight, sel_key_weight, sel_value_weight,
    branch_weight, key_embed, key_inner, key_outer, value_embed, value_inner, value_outer, out_weight, chosen,
):
    tok_rows, width = tokens.shape
    owners = lax.axis_size("kv")
    dev = lax.axis_index("kv")
    tp = lax.axis_index("tp")
    span_queries = tok_rows // Q_BLOCK
    span_blocks = tok_rows // SEL_BLOCK
    cmp_blocks = tok_rows // CMP_BLOCK
    half = span_queries // 2
    picks = chosen[0]
    match = picks // span_blocks == dev
    wanted = jnp.sum(jnp.where(match, picks % span_blocks, 0), axis=1).astype(jnp.int32)
    meta = jnp.concatenate([wanted, jnp.stack([dev, tp]).astype(jnp.int32)])
    my_picks = lax.dynamic_slice_in_dim(picks, dev * span_queries, span_queries, 0)
    source = (my_picks // span_blocks).astype(jnp.int32).reshape(-1)
    own_block = (dev * span_queries + jnp.arange(span_queries, dtype=jnp.int32)) * (Q_BLOCK // SEL_BLOCK)
    bias = jnp.where(my_picks < own_block[:, None], 0.0, MASKED).astype(F32)
    bias = jnp.repeat(bias, SEL_BLOCK, axis=1)[:, None, :]

    coarse, fine = rope_tables(owners * tok_rows)
    steps = tok_rows // TILE
    n_meta = meta.shape[0]
    gates_t = branch_weight.transpose(0, 2, 1).reshape(-1, width)
    tile = lambda: pl.BlockSpec((TILE, LANES), lambda i, m: (i, 0))
    heads_tile = lambda: pl.BlockSpec((2, TILE, LANES), lambda i, m: (0, i, 0))
    slots = lambda n: jax.ShapeDtypeStruct((owners, n, SEL_BLOCK, LANES), BF16)
    qp, qt, kv, gate_cmp, gate_sel, first, second = pl.pallas_call(
        project_kernel,
        grid_spec=pltpu.PrefetchScalarGridSpec(
            num_scalar_prefetch=1,
            grid=(steps,),
            in_specs=[
                pl.BlockSpec((TILE, width), lambda i, m: (i, 0)),
                whole((1, width)),
                whole((width, LANES)),
                whole((HEAD_DIM, width)),
                whole((HEAD_DIM, width)),
                whole((HEAD_DIM, width)),
                whole((HEAD_DIM, width)),
                whole(gates_t.shape),
                pl.BlockSpec((1, 2, LANES), lambda i, m: (m[n_meta - 2] * steps + i, 0, 0)),
                whole((2, TILE, LANES)),
                whole((CMP_BLOCK, HEAD_DIM)),
                whole((HEAD_DIM, CMP_BLOCK * HEAD_DIM)),
                whole((HEAD_DIM, HEAD_DIM)),
                whole((CMP_BLOCK, HEAD_DIM)),
                whole((HEAD_DIM, CMP_BLOCK * HEAD_DIM)),
                whole((HEAD_DIM, HEAD_DIM)),
            ],
            out_specs=[
                heads_tile(), heads_tile(), tile(), tile(), tile(),
                whole((owners, half + 1, SEL_BLOCK, LANES)),
                whole((owners, half, SEL_BLOCK, LANES)),
            ],
            scratch_shapes=[
                pltpu.VMEM((width, 4 * LANES), BF16),
                pltpu.VMEM((span_blocks, SEL_BLOCK, LANES), BF16),
                pltpu.VMEM((tok_rows, LANES), F32),
            ],
        ),
        out_shape=[
            jax.ShapeDtypeStruct((2, tok_rows, LANES), BF16),
            jax.ShapeDtypeStruct((2, tok_rows, LANES), BF16),
            jax.ShapeDtypeStruct((tok_rows, LANES), BF16),
            jax.ShapeDtypeStruct((tok_rows, LANES), F32),
            jax.ShapeDtypeStruct((tok_rows, LANES), F32),
            slots(half + 1),
            slots(half),
        ],
        compiler_params=pltpu.CompilerParams(
            dimension_semantics=("arbitrary",), vmem_limit_bytes=48 * 1024 * 1024
        ),
        name="project",
    )(
        meta, tokens, norm_gain.reshape(1, width), query_weight, sel_key_weight.T, sel_value_weight.T,
        cmp_key_weight.T, cmp_value_weight.T, gates_t, jnp.asarray(coarse), jnp.asarray(fine),
        key_embed[0], key_inner[0].T, key_outer[0], value_embed[0], value_inner[0].T, value_outer[0],
    )
    first = lax.all_to_all(first, "kv", 0, 0, tiled=True)
    second = lax.all_to_all(second, "kv", 0, 0, tiled=True)

    base = (dev * tok_rows).astype(jnp.int32).reshape(1)
    gated = pl.pallas_call(
        compress_kernel,
        grid_spec=pltpu.PrefetchScalarGridSpec(
            num_scalar_prefetch=1,
            grid=(span_queries,),
            in_specs=[
                pl.BlockSpec((2, Q_BLOCK, LANES), lambda i, m: (0, i, 0)),
                pl.BlockSpec((owners, 1, cmp_blocks, LANES), lambda i, m: (0, half, 0, 0)),
                pl.BlockSpec((Q_BLOCK, LANES), lambda i, m: (i, 0)),
            ],
            out_specs=pl.BlockSpec((Q_BLOCK, LANES), lambda i, m: (i, 0)),
            scratch_shapes=[pltpu.VMEM((owners * cmp_blocks, LANES), BF16)],
        ),
        out_shape=jax.ShapeDtypeStruct((tok_rows, LANES), F32),
        compiler_params=pltpu.CompilerParams(
            dimension_semantics=("arbitrary",), vmem_limit_bytes=48 * 1024 * 1024
        ),
        name="compress",
    )(base, qp, first, gate_cmp)

    def select(incoming, parity):
        return pl.pallas_call(
            functools.partial(select_kernel, parity=parity),
            grid_spec=pltpu.PrefetchScalarGridSpec(
                num_scalar_prefetch=1,
                grid=(half,),
                in_specs=[
                    pl.BlockSpec((2, Q_BLOCK, LANES), lambda i, m: (0, 2 * i + parity, 0)),
                    pl.BlockSpec((Q_BLOCK, LANES), lambda i, m: (2 * i + parity, 0)),
                    pl.BlockSpec((owners, 1, SEL_BLOCK, LANES), lambda i, m: (0, i, 0, 0)),
                    pl.BlockSpec((1, 1, FAR_PICKS * SEL_BLOCK), lambda i, m: (2 * i + parity, 0, 0)),
                    pl.BlockSpec((Q_BLOCK, LANES), lambda i, m: (2 * i + parity, 0)),
                    pl.BlockSpec((Q_BLOCK, LANES), lambda i, m: (2 * i + parity, 0)),
                ],
                out_specs=pl.BlockSpec((1, Q_BLOCK, LANES), lambda i, m: (i, 0, 0)),
                scratch_shapes=[
                    pltpu.VMEM((Q_BLOCK + FAR_PICKS * SEL_BLOCK, LANES), BF16),
                    pltpu.VMEM((Q_BLOCK + FAR_PICKS * SEL_BLOCK, LANES), BF16),
                ],
            ),
            out_shape=jax.ShapeDtypeStruct((half, Q_BLOCK, LANES), BF16),
            compiler_params=pltpu.CompilerParams(
                dimension_semantics=("arbitrary",), vmem_limit_bytes=48 * 1024 * 1024
            ),
            name="select",
        )(source, qt, kv, incoming, bias, gate_sel, gated)

    outs = []
    for incoming, parity in ((first, 0), (second, 1)):
        mixed = select(incoming, parity)
        rows = lax.all_to_all(mixed, "tp", 0, 0, tiled=True)
        weight = out_weight.reshape(rows.shape[0], LANES, out_weight.shape[1])
        outs.append(jnp.einsum("trc,tcd->rd", rows, weight, preferred_element_type=F32).astype(BF16))
    return jnp.concatenate(outs, axis=0)


def solution(mesh):
    placed = (
        P("kv", None),
        P(),
        P(None, "tp"),
        P(None, "tp"),
        P(None, "tp"),
        P(None, "tp"),
        P(None, "tp"),
        P(),
        P("tp", None, None),
        P("tp", None, None),
        P("tp", None, None),
        P("tp", None, None),
        P("tp", None, None),
        P("tp", None, None),
        P(),
        P("tp", None, None),
    )
    return jax.shard_map(
        per_device, mesh=mesh, in_specs=placed, out_specs=P(("kv", "tp"), None), check_vma=False
    )
```

```python
import functools

import jax
import jax.numpy as jnp
import numpy as np
from jax import lax
from jax.experimental import pallas as pl
from jax.experimental.pallas import tpu as pltpu
from jax.sharding import PartitionSpec as P

HEAD_DIM = 64
CMP_BLOCK = 32
SEL_BLOCK = 64
Q_BLOCK = 128
FAR_PICKS = 8
ROPE_BASE = 10000.0
NORM_EPS = 1e-06
MASKED = -1e30
LANES = 128
TILE = 256
SPAN_BLOCKS = 32
LOG2E = 1.4426950408889634
TOGETHER = 4

F32 = jnp.float32
BF16 = jnp.bfloat16


def dot_nt(a, b):
    return lax.dot_general(a, b, (((1,), (1,)), ((), ())), preferred_element_type=F32)


def rope_tables(total):
    lane = np.arange(LANES)
    inverse = ROPE_BASE ** (-(lane % 32) / 32.0)
    sign = np.where(lane % 64 < 32, -1.0, 1.0)
    coarse = (np.arange(total // TILE) * TILE)[:, None] * inverse[None, :]
    fine = np.arange(TILE)[:, None] * inverse[None, :]
    pack = lambda a: np.stack([np.cos(a), np.sin(a) * sign[None, :]], axis=1).astype(np.float32)
    return pack(coarse), pack(fine).transpose(1, 0, 2)


def wanted_blocks(picks, dev, span_blocks):
    match = picks // span_blocks == dev
    return jnp.sum(jnp.where(match, picks % span_blocks, 0), axis=0, keepdims=True)


def project_kernel(dev_ref, tp_ref, *refs):
    n_in = 17
    tok_ref, *rest = refs[:n_in]
    coarse_ref = rest.pop(9)
    qp_ref, qt_ref, kv_ref, gc_ref, gs_ref, first_ref = refs[n_in:n_in + 6]
    tok_scr, *local = refs[n_in + 6:2 * n_in + 6]
    coarse_scr = local.pop(9)
    (
        gain_scr, wq_scr, sk_scr, sv_scr, ck_scr, cv_scr, bw_scr, pick_scr, fine_scr,
        ke_scr, ki_scr, ko_scr, ve_scr, vi_scr, vo_scr,
    ) = local
    (
        qp_scr, qt_scr, kv_scr, gc_scr, gs_scr, first_scr, w_scr, raw_scr, inv_scr, c_scr, xk_scr, xv_scr,
        want_vmem, want_smem, tok_sem, in_sem, want_sem, out_sem,
    ) = refs[2 * n_in + 6:]
    tiles = tok_scr.shape[0]
    owners, slots = first_scr.shape[:2]
    half = slots - 1
    span_blocks = kv_scr.shape[0]
    lane = lax.broadcasted_iota(jnp.int32, (TILE, LANES), 1)
    low = lane < HEAD_DIM

    def tile_copy(t):
        return pltpu.make_async_copy(tok_ref.at[pl.ds(t * TILE, TILE), :], tok_scr.at[t], tok_sem.at[t])

    copies = [pltpu.make_async_copy(src, dst, in_sem.at[i]) for i, (src, dst) in enumerate(zip(rest, local))]
    copies.append(
        pltpu.make_async_copy(coarse_ref.at[pl.ds(dev_ref[0] * tiles, tiles)], coarse_scr, in_sem.at[len(local)])
    )
    for copy in copies[:8]:
        copy.start()
    tile_copy(0).start()
    for copy in copies[8:]:
        copy.start()
    for t in range(1, tiles):
        tile_copy(t).start()
    copies[7].wait()
    want_vmem[...] = wanted_blocks(pick_scr[...], dev_ref[0], span_blocks)
    fetch = pltpu.make_async_copy(want_vmem, want_smem, want_sem)
    fetch.start()
    for copy in copies[:7]:
        copy.wait()
    rows = gain_scr[...]
    gain = jnp.concatenate([rows[k:k + 1, :] for k in range(rows.shape[0])], axis=1)
    gain_cols = jnp.broadcast_to(gain, (LANES, gain.shape[1])).T
    w_scr[:, 0:LANES] = (wq_scr[...].astype(F32) * gain_cols.astype(F32)).astype(BF16)
    gain = gain.astype(F32)
    scaled = lambda ref: (ref[...].astype(F32) * gain).astype(BF16)
    w_scr[:, LANES:2 * LANES] = jnp.concatenate([scaled(sk_scr), scaled(sv_scr)], axis=0).T
    w_scr[:, 2 * LANES:3 * LANES] = jnp.concatenate([scaled(ck_scr), scaled(cv_scr)], axis=0).T
    bw = scaled(bw_scr)
    pad = jnp.zeros((LANES - bw.shape[0], bw.shape[1]), BF16)
    w_scr[:, 3 * LANES:4 * LANES] = jnp.concatenate([bw, pad], axis=0).T
    for copy in copies[8:]:
        copy.wait()

    first_half = (lane % HEAD_DIM) < 32
    blocks = TILE // CMP_BLOCK
    low_b = lax.broadcasted_iota(jnp.int32, (blocks, LANES), 1) < HEAD_DIM
    per = TILE // SEL_BLOCK

    def out_copies(t):
        at = pl.ds(pl.multiple_of(t * TILE, TILE), TILE)
        pairs = (
            (qp_scr.at[:, at, :], qp_ref.at[:, at, :]),
            (qt_scr.at[:, at, :], qt_ref.at[:, at, :]),
            (kv_scr.at[pl.ds(t * per, per)], kv_ref.at[pl.ds(t * per, per)]),
            (gc_scr.at[at, :], gc_ref.at[at, :]),
            (gs_scr.at[at, :], gs_ref.at[at, :]),
        )
        return [pltpu.make_async_copy(src, dst, out_sem.at[i]) for i, (src, dst) in enumerate(pairs)]

    def tile(step, carry):
        prev = jnp.maximum(step - 1, 0)
        now = jnp.minimum(step, tiles - 1)
        raw = raw_scr[...]
        inv = inv_scr[...]

        @pl.when(step < tiles)
        def _():
            tile_copy(now).wait()

        fresh = jnp.dot(tok_scr[now], w_scr[...], preferred_element_type=F32)
        squares = jnp.zeros((TILE, LANES), F32)
        for k in range(tok_scr.shape[2] // LANES):
            part = tok_scr[now, :, k * LANES:(k + 1) * LANES].astype(F32)
            squares = squares + part * part
        mean = jnp.sum(squares, axis=-1, keepdims=True) * (1.0 / tok_scr.shape[2])

        ch = coarse_scr[prev, 0:1, :]
        sh = coarse_scr[prev, 1:2, :]
        cl = fine_scr[0]
        sl = fine_scr[1]
        cosine = ch * cl - sh * sl
        sine = sh * cl + ch * sl

        def turn(v):
            swapped = jnp.where(first_half, pltpu.roll(v, LANES - 32, 1), pltpu.roll(v, 32, 1))
            return v * cosine + swapped * sine

        at = pl.ds(pl.multiple_of(prev * TILE, TILE), TILE)
        q = raw[:, 0:LANES] * (inv * (HEAD_DIM ** (-0.5) * LOG2E))
        turned = turn(q)
        qp_scr[0, at, :] = jnp.where(low, q, 0.0).astype(BF16)
        qp_scr[1, at, :] = jnp.where(low, pltpu.roll(q, HEAD_DIM, 1), 0.0).astype(BF16)
        qt_scr[0, at, :] = jnp.where(low, turned, 0.0).astype(BF16)
        qt_scr[1, at, :] = jnp.where(low, pltpu.roll(turned, HEAD_DIM, 1), 0.0).astype(BF16)
        kv = raw[:, LANES:2 * LANES] * inv
        kv = jnp.where(low, turn(kv), kv).astype(BF16)
        kv_scr[pl.ds(prev * per, per)] = kv.reshape(per, SEL_BLOCK, LANES)
        c_scr[...] = (raw[:, 2 * LANES:3 * LANES] * inv).astype(BF16).astype(F32)
        logits = pltpu.roll(raw[:, 3 * LANES:4 * LANES] * inv, LANES - tp_ref[0] * 2, 1)
        gates = 1.0 / (1.0 + jnp.exp(-logits))
        gc_scr[at, :] = jnp.where(low, gates[:, 0:1], gates[:, 1:2])
        gs_scr[at, :] = jnp.where(low, gates[:, 16:17], gates[:, 17:18])

        embed = jnp.concatenate([ke_scr[...], ve_scr[...]], axis=1).astype(F32)
        part = pl.ds(pl.multiple_of(prev * blocks, blocks), blocks)
        for pair in range(CMP_BLOCK // 2):
            r = 2 * pair
            a = c_scr[pl.ds(r, blocks, stride=CMP_BLOCK), :] + embed[r:r + 1, :]
            b = c_scr[pl.ds(r + 1, blocks, stride=CMP_BLOCK), :] + embed[r + 1:r + 2, :]
            cols = slice(pair * LANES, (pair + 1) * LANES)
            xk_scr[part, cols] = jnp.where(low_b, a, pltpu.roll(b, HEAD_DIM, 1))
            xv_scr[part, cols] = jnp.where(low_b, pltpu.roll(a, HEAD_DIM, 1), b)
        raw_scr[...] = fresh
        inv_scr[...] = lax.rsqrt(mean + NORM_EPS)

        @pl.when(step > 0)
        def _():
            for copy in out_copies(prev):
                copy.start()

        return carry

    lax.fori_loop(0, tiles + 1, tile, 0)
    fetch.wait()
    hidden_k = jax.nn.gelu(dot_nt(xk_scr[...].astype(BF16), ki_scr[...])).astype(BF16)
    hidden_v = jax.nn.gelu(dot_nt(xv_scr[...].astype(BF16), vi_scr[...])).astype(BF16)
    summary = jnp.concatenate(
        [
            jnp.dot(hidden_k, ko_scr[...], preferred_element_type=F32),
            jnp.dot(hidden_v, vo_scr[...], preferred_element_type=F32),
        ],
        axis=1,
    ).astype(BF16)

    def fill(d, carry):
        for j in range(half):
            first_scr[d, j] = kv_scr[want_smem[0, d * 2 * half + 2 * j]]
        first_scr[d, half] = summary
        pltpu.make_async_copy(first_scr.at[d], first_ref.at[d], out_sem.at[5]).start()
        return carry

    lax.fori_loop(0, owners, fill, 0)
    pairs = (
        (qp_scr, qp_ref), (qt_scr, qt_ref), (kv_scr, kv_ref), (gc_scr, gc_ref), (gs_scr, gs_ref),
        (first_scr, first_ref),
    )
    for i, (src, dst) in enumerate(pairs):
        pltpu.make_async_copy(src, dst, out_sem.at[i]).wait()


def pack_kernel(dev_ref, pick_ref, kv_ref, out_ref, out_scr, want_vmem, want_smem, want_sem, out_sem):
    want_vmem[...] = wanted_blocks(pick_ref[...], dev_ref[0], kv_ref.shape[0])
    fetch = pltpu.make_async_copy(want_vmem, want_smem, want_sem)
    fetch.start()
    fetch.wait()
    owners, half = out_scr.shape[:2]

    def fill(d, carry):
        for j in range(half):
            out_scr[d, j] = kv_ref[want_smem[0, d * 2 * half + 2 * j + 1]]
        pltpu.make_async_copy(out_scr.at[d], out_ref.at[d], out_sem).start()
        return carry

    lax.fori_loop(0, owners, fill, 0)
    pltpu.make_async_copy(out_scr, out_ref, out_sem).wait()


def heads_to_lanes(out):
    rows = out.shape[1] // 2
    return jnp.concatenate([out[:, :rows], out[:, rows:]], axis=0).T


def compress_kernel(dev_ref, qp_ref, sum_ref, gc_ref, out_ref, k_scr, v_scr):
    owners, _, blocks, _ = sum_ref.shape
    count = owners * blocks
    dev = dev_ref[0]
    step = pl.program_id(0)

    @pl.when(step == 0)
    def _():
        lane = lax.broadcasted_iota(jnp.int32, (blocks, LANES), 1)
        for slot in range(owners):
            span = jnp.where(slot == 0, dev, jnp.where(slot == dev, 0, slot))
            rows = slice(slot * blocks, (slot + 1) * blocks)
            pair = sum_ref[span, 0].astype(F32)
            hide = jnp.where(span <= dev, 0.0, MASKED)
            k_scr[rows, :] = jnp.where(lane < HEAD_DIM, pair, jnp.where(lane == HEAD_DIM, hide, 0.0)).astype(BF16)
            v_scr[:, rows] = pair.T[HEAD_DIM:, :].astype(BF16)

    size = qp_ref.shape[1]
    lane = lax.broadcasted_iota(jnp.int32, (2 * size, LANES), 1)
    col = lax.broadcasted_iota(jnp.int32, (1, 2 * size), 1) % size
    own = lax.broadcasted_iota(jnp.int32, (blocks, 2 * size), 0)
    limit = (step * size + col + 1) // CMP_BLOCK
    q = qp_ref[...].reshape(2 * size, LANES)
    q = jnp.where(lane == HEAD_DIM, 1.0, q.astype(F32)).astype(BF16)
    scores = dot_nt(k_scr[...], q)
    near = jnp.where(own < limit, scores[:blocks], MASKED)
    scores = jnp.concatenate([near, scores[blocks:]], axis=0)
    top = jnp.max(scores, axis=0, keepdims=True)
    probs = jnp.exp2(scores - top)
    total = jnp.sum(probs, axis=0, keepdims=True)
    out = jnp.dot(v_scr[...], probs.astype(BF16), preferred_element_type=F32)
    out = jnp.where((limit > 0) | (dev > 0), out / total, 0.0)
    out_ref[...] = gc_ref[...] * heads_to_lanes(out)


def select_kernel(
    dev_ref, pick_ref, qt_ref, kv_ref, in_ref, gs_ref, cmp_ref, out_ref,
    q_scr, k_scr, gs_scr, cmp_scr, o_scr, pick_sem, sem, out_sem, *, parity
):
    count = out_ref.shape[0]
    dev = dev_ref[0]
    first = dev * 2 * count + parity

    def start(block, carry):
        for j in range(FAR_PICKS):
            span = pick_ref[j, first + 2 * block] // SPAN_BLOCKS
            rows = pl.ds(Q_BLOCK + j * SEL_BLOCK, SEL_BLOCK)
            pltpu.make_async_copy(in_ref.at[span, block], k_scr.at[block, rows, :], pick_sem.at[block]).start()
        return carry

    own_rows = k_scr.at[:, pl.ds(0, Q_BLOCK), :]
    early = [
        pltpu.make_async_copy(qt_ref.at[:, :, parity], q_scr, sem.at[0]),
        pltpu.make_async_copy(kv_ref.at[:, parity], own_rows, sem.at[1]),
    ]
    late = [
        pltpu.make_async_copy(gs_ref.at[:, parity], gs_scr, sem.at[2]),
        pltpu.make_async_copy(cmp_ref.at[:, parity], cmp_scr, sem.at[3]),
    ]
    for copy in early:
        copy.start()
    lax.fori_loop(0, count, start, 0)
    for copy in late:
        copy.start()
    for copy in early:
        copy.wait()
    low = lax.broadcasted_iota(jnp.int32, (Q_BLOCK, LANES), 1) < HEAD_DIM
    row = lax.broadcasted_iota(jnp.int32, (2 * Q_BLOCK, Q_BLOCK), 0) % Q_BLOCK
    causal = lax.broadcasted_iota(jnp.int32, (2 * Q_BLOCK, Q_BLOCK), 1) <= row
    far_keys = FAR_PICKS * SEL_BLOCK
    pick_of = lax.broadcasted_iota(jnp.int32, (1, far_keys), 1) // SEL_BLOCK
    low_k = lax.broadcasted_iota(jnp.int32, (Q_BLOCK + far_keys, LANES), 1) < HEAD_DIM

    def body(group, carry):
        scored = []
        for u in range(TOGETHER):
            block = group * TOGETHER + u
            far = k_scr.at[block, pl.ds(Q_BLOCK, far_keys), :]
            pltpu.make_async_copy(far, far, pick_sem.at[block]).wait()
        for u in range(TOGETHER):
            block = group * TOGETHER + u
            keys = k_scr[block]
            scored.append((block, keys, dot_nt(q_scr[:, block].reshape(2 * Q_BLOCK, LANES), keys)))
        weighed = []
        for block, keys, scores in scored:
            index = first + 2 * block
            bias = jnp.zeros((1, far_keys), F32)
            for j in range(FAR_PICKS):
                later = pick_ref[j, index] >= index * (Q_BLOCK // SEL_BLOCK)
                bias = jnp.where(pick_of == j, jnp.where(later, MASKED, 0.0), bias)
            own = jnp.where(causal, scores[:, :Q_BLOCK], MASKED)
            scores = jnp.concatenate([own, scores[:, Q_BLOCK:] + bias], axis=1)
            top = jnp.max(scores, axis=1, keepdims=True)
            weighed.append((block, keys, jnp.exp2(scores - top).astype(BF16)))

        @pl.when(group == 0)
        def _():
            for copy in late:
                copy.wait()

        for block, keys, probs in weighed:
            values = jnp.where(low_k, 1.0, keys.astype(F32)).astype(BF16)
            mixed = jnp.dot(probs, values, preferred_element_type=F32)
            out = mixed / pltpu.roll(mixed, HEAD_DIM, 1)
            joined = jnp.where(low, pltpu.roll(out[:Q_BLOCK], HEAD_DIM, 1), out[Q_BLOCK:])
            o_scr[block] = (cmp_scr[block] + gs_scr[block] * joined).astype(BF16)
            pltpu.make_async_copy(o_scr.at[block], out_ref.at[block], out_sem).start()
        return carry

    lax.fori_loop(0, count // TOGETHER, body, 0)
    pltpu.make_async_copy(o_scr, out_ref, out_sem).wait()


def whole(shape):
    return pl.BlockSpec(shape, lambda i, *_: (0,) * len(shape))


def per_device(
    tokens, norm_gain, query_weight, cmp_key_weight, cmp_value_weight, sel_key_weight, sel_value_weight,
    branch_weight, key_embed, key_inner, key_outer, value_embed, value_inner, value_outer, out_weight, chosen,
):
    tok_rows, width = tokens.shape
    owners = lax.axis_size("kv")
    dev = lax.axis_index("kv")
    tp = lax.axis_index("tp")
    span_queries = tok_rows // Q_BLOCK
    span_blocks = tok_rows // SEL_BLOCK
    cmp_blocks = tok_rows // CMP_BLOCK
    half = span_queries // 2
    picks = chosen[0].T
    dev = dev.astype(jnp.int32).reshape(1)
    tp = tp.astype(jnp.int32).reshape(1)

    coarse, fine = rope_tables(owners * tok_rows)
    steps = tok_rows // TILE
    gates_t = branch_weight.transpose(0, 2, 1).reshape(-1, width)
    slots = lambda n: jax.ShapeDtypeStruct((owners, n, SEL_BLOCK, LANES), BF16)
    inputs = [
        tokens, norm_gain.reshape(-1, LANES), query_weight, sel_key_weight.T, sel_value_weight.T,
        cmp_key_weight.T, cmp_value_weight.T, gates_t, picks, jnp.asarray(fine), jnp.asarray(coarse),
        key_embed[0], key_inner[0].T, key_outer[0], value_embed[0], value_inner[0].T, value_outer[0],
    ]
    outputs = [
        jax.ShapeDtypeStruct((2, tok_rows, LANES), BF16),
        jax.ShapeDtypeStruct((2, tok_rows, LANES), BF16),
        jax.ShapeDtypeStruct((span_blocks, SEL_BLOCK, LANES), BF16),
        jax.ShapeDtypeStruct((tok_rows, LANES), F32),
        jax.ShapeDtypeStruct((tok_rows, LANES), F32),
        slots(half + 1),
    ]
    local = [pltpu.VMEM(v.shape, v.dtype) for v in inputs]
    local[0] = pltpu.VMEM((steps, TILE, width), BF16)
    local[10] = pltpu.VMEM((steps, 2, LANES), F32)
    any_space = pl.BlockSpec(memory_space=pl.ANY)
    big = pltpu.CompilerParams(dimension_semantics=("arbitrary",), vmem_limit_bytes=67_043_328)
    qp, qt, kv, gate_cmp, gate_sel, first = pl.pallas_call(
        project_kernel,
        grid_spec=pltpu.PrefetchScalarGridSpec(
            num_scalar_prefetch=2,
            grid=(1,),
            in_specs=[any_space] * len(inputs),
            out_specs=[any_space] * len(outputs),
            scratch_shapes=[
                *local,
                *[pltpu.VMEM(v.shape, v.dtype) for v in outputs],
                pltpu.VMEM((width, 4 * LANES), BF16),
                pltpu.VMEM((TILE, 4 * LANES), F32),
                pltpu.VMEM((TILE, 1), F32),
                pltpu.VMEM((TILE, LANES), F32),
                pltpu.VMEM((cmp_blocks, CMP_BLOCK * HEAD_DIM), F32),
                pltpu.VMEM((cmp_blocks, CMP_BLOCK * HEAD_DIM), F32),
                pltpu.VMEM((1, picks.shape[1]), jnp.int32),
                pltpu.SMEM((1, picks.shape[1]), jnp.int32),
                pltpu.SemaphoreType.DMA((steps,)),
                pltpu.SemaphoreType.DMA((len(inputs) - 1,)),
                pltpu.SemaphoreType.DMA,
                pltpu.SemaphoreType.DMA((len(outputs),)),
            ],
        ),
        out_shape=outputs,
        compiler_params=big,
        name="project",
    )(dev, tp, *inputs)
    second = pl.pallas_call(
        pack_kernel,
        grid_spec=pltpu.PrefetchScalarGridSpec(
            num_scalar_prefetch=1,
            grid=(1,),
            in_specs=[whole(picks.shape), whole(kv.shape)],
            out_specs=any_space,
            scratch_shapes=[
                pltpu.VMEM((owners, half, SEL_BLOCK, LANES), BF16),
                pltpu.VMEM((1, picks.shape[1]), jnp.int32),
                pltpu.SMEM((1, picks.shape[1]), jnp.int32),
                pltpu.SemaphoreType.DMA,
                pltpu.SemaphoreType.DMA,
            ],
        ),
        out_shape=slots(half),
        compiler_params=big,
        name="pack",
    )(dev, picks, kv)
    first = lax.all_to_all(first, "kv", 0, 0, tiled=True)
    second = lax.all_to_all(second, "kv", 0, 0, tiled=True)

    gated = pl.pallas_call(
        compress_kernel,
        grid_spec=pltpu.PrefetchScalarGridSpec(
            num_scalar_prefetch=1,
            grid=(4,),
            in_specs=[
                pl.BlockSpec((2, tok_rows // 4, LANES), lambda i, *m: (0, i, 0)),
                pl.BlockSpec((owners, 1, cmp_blocks, LANES), lambda i, *m: (0, half, 0, 0)),
                pl.BlockSpec((tok_rows // 4, LANES), lambda i, *m: (i, 0)),
            ],
            out_specs=pl.BlockSpec((tok_rows // 4, LANES), lambda i, *m: (i, 0)),
            scratch_shapes=[
                pltpu.VMEM((owners * cmp_blocks, LANES), BF16),
                pltpu.VMEM((HEAD_DIM, owners * cmp_blocks), BF16),
            ],
        ),
        out_shape=jax.ShapeDtypeStruct((tok_rows, LANES), F32),
        compiler_params=pltpu.CompilerParams(
            dimension_semantics=("arbitrary",), vmem_limit_bytes=67_043_328
        ),
        name="compress",
    )(dev, qp, first, gate_cmp)

    by_parity = lambda v: v.reshape(half, 2, Q_BLOCK, LANES)

    def select(incoming, parity):
        return pl.pallas_call(
            functools.partial(select_kernel, parity=parity),
            grid_spec=pltpu.PrefetchScalarGridSpec(
                num_scalar_prefetch=2,
                grid=(1,),
                in_specs=[pl.BlockSpec(memory_space=pl.ANY)] * 5,
                out_specs=pl.BlockSpec(memory_space=pl.ANY),
                scratch_shapes=[
                    pltpu.VMEM((2, half, Q_BLOCK, LANES), BF16),
                    pltpu.VMEM((half, Q_BLOCK + FAR_PICKS * SEL_BLOCK, LANES), BF16),
                    pltpu.VMEM((half, Q_BLOCK, LANES), F32),
                    pltpu.VMEM((half, Q_BLOCK, LANES), F32),
                    pltpu.VMEM((half, Q_BLOCK, LANES), BF16),
                    pltpu.SemaphoreType.DMA((half,)),
                    pltpu.SemaphoreType.DMA((4,)),
                    pltpu.SemaphoreType.DMA,
                ],
            ),
            out_shape=jax.ShapeDtypeStruct((half, Q_BLOCK, LANES), BF16),
            compiler_params=pltpu.CompilerParams(
                dimension_semantics=("arbitrary",), vmem_limit_bytes=67_043_328
            ),
            name="select",
        )(
            dev, picks, qt.reshape(2, half, 2, Q_BLOCK, LANES), by_parity(kv), incoming,
            by_parity(gate_sel), by_parity(gated),
        )

    outs = []
    for incoming, parity in ((first, 0), (second, 1)):
        mixed = select(incoming, parity)
        rows = lax.all_to_all(mixed, "tp", 0, 0, tiled=True)
        weight = out_weight.reshape(rows.shape[0], LANES, out_weight.shape[1])
        outs.append(jnp.einsum("trc,tcd->rd", rows, weight, preferred_element_type=F32).astype(BF16))
    return jnp.concatenate(outs, axis=0)


def solution(mesh):
    placed = (
        P("kv", None),
        P(),
        P(None, "tp"),
        P(None, "tp"),
        P(None, "tp"),
        P(None, "tp"),
        P(None, "tp"),
        P(),
        P("tp", None, None),
        P("tp", None, None),
        P("tp", None, None),
        P("tp", None, None),
        P("tp", None, None),
        P("tp", None, None),
        P(),
        P("tp", None, None),
    )
    return jax.shard_map(
        per_device, mesh=mesh, in_specs=placed, out_specs=P(("kv", "tp"), None), check_vma=False
    )
```

```python
import functools

import jax
import jax.numpy as jnp
import numpy as np
from jax import lax
from jax.experimental import pallas as pl
from jax.experimental.pallas import tpu as pltpu
from jax.sharding import PartitionSpec as P

HEAD_DIM = 64
CMP_BLOCK = 32
SEL_BLOCK = 64
Q_BLOCK = 128
FAR_PICKS = 8
ROPE_BASE = 10000.0
NORM_EPS = 1e-06
MASKED = -1e30
LANES = 128
TILE = 256
SPAN_BLOCKS = 32
HALF = SEL_BLOCK // 2
SIDE = 4
LOG2E = 1.4426950408889634
TOGETHER = 4

F32 = jnp.float32
BF16 = jnp.bfloat16


def dot_nt(a, b):
    return lax.dot_general(a, b, (((1,), (1,)), ((), ())), preferred_element_type=F32)


def rope_tables(total):
    lane = np.arange(LANES)
    inverse = ROPE_BASE ** (-(lane % 32) / 32.0)
    sign = np.where(lane % 64 < 32, -1.0, 1.0)
    coarse = (np.arange(total // TILE) * TILE)[:, None] * inverse[None, :]
    fine = np.arange(TILE)[:, None] * inverse[None, :]
    pack = lambda a: np.stack([np.cos(a), np.sin(a) * sign[None, :]], axis=1).astype(np.float32)
    return pack(coarse), pack(fine).transpose(1, 0, 2)


def wanted_blocks(picks, dev, span_blocks):
    match = picks // span_blocks == dev
    return jnp.sum(jnp.where(match, picks % span_blocks, 0), axis=0, keepdims=True)


def project_kernel(dev_ref, tp_ref, *refs):
    n_in = 16
    tok_ref, *rest = refs[:n_in]
    coarse_ref = rest.pop(8)
    qp_ref, qt_ref, kv_ref, gc_ref, gs_ref, top_ref, bot_ref = refs[n_in:n_in + 7]
    tok_scr, *local = refs[n_in + 7:2 * n_in + 7]
    coarse_scr = local.pop(8)
    (
        gain_scr, wq_scr, sk_scr, sv_scr, ck_scr, cv_scr, bw_scr, fine_scr,
        ke_scr, ki_scr, ko_scr, ve_scr, vi_scr, vo_scr,
    ) = local
    (
        qp_scr, qt_scr, kv_scr, gc_scr, gs_scr, sum_scr, w_scr, raw_scr, inv_scr, c_scr, xk_scr, xv_scr,
        tok_sem, in_sem, out_sem,
    ) = refs[2 * n_in + 7:]
    tiles = tok_scr.shape[0]
    span_blocks = kv_scr.shape[0]
    lane = lax.broadcasted_iota(jnp.int32, (TILE, LANES), 1)
    low = lane < HEAD_DIM

    def tile_copy(t):
        return pltpu.make_async_copy(tok_ref.at[pl.ds(t * TILE, TILE), :], tok_scr.at[t], tok_sem.at[t])

    copies = [pltpu.make_async_copy(src, dst, in_sem.at[i]) for i, (src, dst) in enumerate(zip(rest, local))]
    copies.append(
        pltpu.make_async_copy(coarse_ref.at[pl.ds(dev_ref[0] * tiles, tiles)], coarse_scr, in_sem.at[len(local)])
    )
    for copy in copies[:7]:
        copy.start()
    tile_copy(0).start()
    for copy in copies[7:]:
        copy.start()
    for t in range(1, tiles):
        tile_copy(t).start()
    for copy in copies[:7]:
        copy.wait()
    rows = gain_scr[...]
    gain = jnp.concatenate([rows[k:k + 1, :] for k in range(rows.shape[0])], axis=1)
    gain_cols = jnp.broadcast_to(gain, (LANES, gain.shape[1])).T
    w_scr[:, 0:LANES] = (wq_scr[...].astype(F32) * gain_cols.astype(F32)).astype(BF16)
    gain = gain.astype(F32)
    scaled = lambda ref: (ref[...].astype(F32) * gain).astype(BF16)
    w_scr[:, LANES:2 * LANES] = jnp.concatenate([scaled(sk_scr), scaled(sv_scr)], axis=0).T
    w_scr[:, 2 * LANES:3 * LANES] = jnp.concatenate([scaled(ck_scr), scaled(cv_scr)], axis=0).T
    bw = scaled(bw_scr)
    pad = jnp.zeros((LANES - bw.shape[0], bw.shape[1]), BF16)
    w_scr[:, 3 * LANES:4 * LANES] = jnp.concatenate([bw, pad], axis=0).T
    for copy in copies[7:]:
        copy.wait()

    first_half = (lane % HEAD_DIM) < 32
    blocks = TILE // CMP_BLOCK
    low_b = lax.broadcasted_iota(jnp.int32, (blocks, LANES), 1) < HEAD_DIM
    per = TILE // SEL_BLOCK

    def out_copies(t):
        at = pl.ds(pl.multiple_of(t * TILE, TILE), TILE)
        pairs = (
            (qp_scr.at[:, at, :], qp_ref.at[:, at, :]),
            (qt_scr.at[:, at, :], qt_ref.at[:, at, :]),
            (kv_scr.at[pl.ds(t * per, per)], kv_ref.at[pl.ds(t * per, per)]),
            (gc_scr.at[at, :], gc_ref.at[at, :]),
            (gs_scr.at[at, :], gs_ref.at[at, :]),
            (kv_scr.at[pl.ds(t * per, per), 0:HALF], top_ref.at[pl.ds(t * per, per)]),
            (kv_scr.at[pl.ds(t * per, per), HALF:SEL_BLOCK], bot_ref.at[pl.ds(t * per, per)]),
        )
        return [pltpu.make_async_copy(src, dst, out_sem.at[i]) for i, (src, dst) in enumerate(pairs)]

    def tile(step, carry):
        prev = jnp.maximum(step - 1, 0)
        now = jnp.minimum(step, tiles - 1)
        raw = raw_scr[...]
        inv = inv_scr[...]

        @pl.when(step < tiles)
        def _():
            tile_copy(now).wait()

        fresh = jnp.dot(tok_scr[now], w_scr[...], preferred_element_type=F32)
        squares = jnp.zeros((TILE, LANES), F32)
        for k in range(tok_scr.shape[2] // LANES):
            part = tok_scr[now, :, k * LANES:(k + 1) * LANES].astype(F32)
            squares = squares + part * part
        mean = jnp.sum(squares, axis=-1, keepdims=True) * (1.0 / tok_scr.shape[2])

        ch = coarse_scr[prev, 0:1, :]
        sh = coarse_scr[prev, 1:2, :]
        cl = fine_scr[0]
        sl = fine_scr[1]
        cosine = ch * cl - sh * sl
        sine = sh * cl + ch * sl

        def turn(v):
            swapped = jnp.where(first_half, pltpu.roll(v, LANES - 32, 1), pltpu.roll(v, 32, 1))
            return v * cosine + swapped * sine

        at = pl.ds(pl.multiple_of(prev * TILE, TILE), TILE)
        q = raw[:, 0:LANES] * (inv * (HEAD_DIM ** (-0.5) * LOG2E))
        turned = turn(q)
        qp_scr[0, at, :] = jnp.where(low, q, 0.0).astype(BF16)
        qp_scr[1, at, :] = jnp.where(low, pltpu.roll(q, HEAD_DIM, 1), 0.0).astype(BF16)
        qt_scr[0, at, :] = jnp.where(low, turned, 0.0).astype(BF16)
        qt_scr[1, at, :] = jnp.where(low, pltpu.roll(turned, HEAD_DIM, 1), 0.0).astype(BF16)
        kv = raw[:, LANES:2 * LANES] * inv
        kv = jnp.where(low, turn(kv), kv).astype(BF16)
        kv_scr[pl.ds(prev * per, per)] = kv.reshape(per, SEL_BLOCK, LANES)
        c_scr[...] = (raw[:, 2 * LANES:3 * LANES] * inv).astype(BF16).astype(F32)
        logits = pltpu.roll(raw[:, 3 * LANES:4 * LANES] * inv, LANES - tp_ref[0] * 2, 1)
        gates = 1.0 / (1.0 + jnp.exp(-logits))
        gc_scr[at, :] = jnp.where(low, gates[:, 0:1], gates[:, 1:2])
        gs_scr[at, :] = jnp.where(low, gates[:, 16:17], gates[:, 17:18])

        embed = jnp.concatenate([ke_scr[...], ve_scr[...]], axis=1).astype(F32)
        part = pl.ds(pl.multiple_of(prev * blocks, blocks), blocks)
        for pair in range(CMP_BLOCK // 2):
            r = 2 * pair
            a = c_scr[pl.ds(r, blocks, stride=CMP_BLOCK), :] + embed[r:r + 1, :]
            b = c_scr[pl.ds(r + 1, blocks, stride=CMP_BLOCK), :] + embed[r + 1:r + 2, :]
            cols = slice(pair * LANES, (pair + 1) * LANES)
            xk_scr[part, cols] = jnp.where(low_b, a, pltpu.roll(b, HEAD_DIM, 1))
            xv_scr[part, cols] = jnp.where(low_b, pltpu.roll(a, HEAD_DIM, 1), b)
        raw_scr[...] = fresh
        inv_scr[...] = lax.rsqrt(mean + NORM_EPS)

        @pl.when(step > 0)
        def _():
            for copy in out_copies(prev):
                copy.start()

        return carry

    lax.fori_loop(0, tiles + 1, tile, 0)
    hidden_k = jax.nn.gelu(dot_nt(xk_scr[...].astype(BF16), ki_scr[...])).astype(BF16)
    hidden_v = jax.nn.gelu(dot_nt(xv_scr[...].astype(BF16), vi_scr[...])).astype(BF16)
    summary = jnp.concatenate(
        [
            jnp.dot(hidden_k, ko_scr[...], preferred_element_type=F32),
            jnp.dot(hidden_v, vo_scr[...], preferred_element_type=F32),
        ],
        axis=1,
    ).astype(BF16)

    sum_scr[...] = summary.reshape(sum_scr.shape)
    tail = pltpu.make_async_copy(sum_scr, top_ref.at[pl.ds(span_blocks, sum_scr.shape[0])], out_sem.at[7])
    tail.start()
    tail.wait()
    halves = top_ref.at[pl.ds(0, span_blocks)]
    pairs = (
        (qp_scr, qp_ref), (qt_scr, qt_ref), (kv_scr, kv_ref), (gc_scr, gc_ref), (gs_scr, gs_ref),
        (kv_scr.at[:, 0:HALF], halves), (kv_scr.at[:, HALF:SEL_BLOCK], bot_ref),
    )
    for i, (src, dst) in enumerate(pairs):
        pltpu.make_async_copy(src, dst, out_sem.at[i]).wait()


def column_kernel(*refs):
    top_refs, (out_ref, sem) = refs[:SIDE], refs[SIDE:]
    count = out_ref.shape[0] // SIDE
    copies = []
    for k, ref in enumerate(top_refs):
        source = ref.at[pl.ds(ref.shape[0] - count, count)]
        copies.append(pltpu.make_async_copy(source, out_ref.at[pl.ds(k * count, count)], sem.at[k]))
    for copy in copies:
        copy.start()
    for copy in copies:
        copy.wait()


def pack_kernel(dev_ref, pick_ref, *refs):
    top_refs, bot_refs, out_refs = refs[:SIDE], refs[SIDE:2 * SIDE], refs[2 * SIDE:4 * SIDE]
    out_scr, want_vmem, want_smem, want_sem, out_sem = refs[4 * SIDE:]
    dev = dev_ref[0]
    z, x = dev // SIDE, dev % SIDE
    picks = pick_ref[...]
    span_blocks = bot_refs[0].shape[0]
    for k in range(SIDE):
        want_vmem[k:k + 1, :] = wanted_blocks(picks, (z - k) % SIDE * SIDE + x, span_blocks)
        want_vmem[SIDE + k:SIDE + k + 1, :] = wanted_blocks(picks, z * SIDE + (x - k) % SIDE, span_blocks)
    fetch = pltpu.make_async_copy(want_vmem, want_smem, want_sem)
    fetch.start()
    fetch.wait()
    queries = out_scr.shape[1]
    for side in range(2):
        sources = (top_refs, bot_refs)[side]
        for m in range(SIDE):
            slot = side * SIDE + m
            dest = z * SIDE + (x + m) % SIDE if side == 0 else (z + m) % SIDE * SIDE + x

            def fill(n, carry):
                for k in range(SIDE):
                    out_scr[slot, n, k] = sources[k][want_smem[side * SIDE + k, dest * queries + n]]
                return carry

            lax.fori_loop(0, queries, fill, 0)
            pltpu.make_async_copy(out_scr.at[slot], out_refs[slot], out_sem.at[slot]).start()
    for slot in range(2 * SIDE):
        pltpu.make_async_copy(out_scr.at[slot], out_refs[slot], out_sem.at[slot]).wait()


def heads_to_lanes(out):
    rows = out.shape[1] // 2
    return jnp.concatenate([out[:, :rows], out[:, rows:]], axis=0).T


def compress_kernel(dev_ref, qp_ref, gc_ref, *refs):
    sum_refs, (out_ref, k_scr, v_scr) = refs[:SIDE], refs[SIDE:]
    count = k_scr.shape[0]
    blocks = count // SIDE // SIDE
    dev = dev_ref[0]
    z, x = dev // SIDE, dev % SIDE
    step = pl.program_id(0)

    @pl.when(step == 0)
    def _():
        lane = lax.broadcasted_iota(jnp.int32, (blocks, LANES), 1)
        for a in range(SIDE):
            for b in range(SIDE):
                slot = a * SIDE + b
                rows = slice(slot * blocks, (slot + 1) * blocks)
                span = (z - b) % SIDE * SIDE + (x - a) % SIDE
                pair = sum_refs[a][2 * b:2 * b + 2].reshape(blocks, LANES).astype(F32)
                hide = jnp.where(span <= dev, 0.0, MASKED)
                k_scr[rows, :] = jnp.where(
                    lane < HEAD_DIM, pair, jnp.where(lane == HEAD_DIM, hide, 0.0)
                ).astype(BF16)
                v_scr[:, rows] = pair.T[HEAD_DIM:, :].astype(BF16)

    size = qp_ref.shape[1]
    lane = lax.broadcasted_iota(jnp.int32, (2 * size, LANES), 1)
    col = lax.broadcasted_iota(jnp.int32, (1, 2 * size), 1) % size
    own = lax.broadcasted_iota(jnp.int32, (blocks, 2 * size), 0)
    limit = (step * size + col + 1) // CMP_BLOCK
    q = qp_ref[...].reshape(2 * size, LANES)
    q = jnp.where(lane == HEAD_DIM, 1.0, q.astype(F32)).astype(BF16)
    scores = dot_nt(k_scr[...], q)
    near = jnp.where(own < limit, scores[:blocks], MASKED)
    scores = jnp.concatenate([near, scores[blocks:]], axis=0)
    top = jnp.max(scores, axis=0, keepdims=True)
    probs = jnp.exp2(scores - top)
    total = jnp.sum(probs, axis=0, keepdims=True)
    out = jnp.dot(v_scr[...], probs.astype(BF16), preferred_element_type=F32)
    out = jnp.where((limit > 0) | (dev > 0), out / total, 0.0)
    out_ref[...] = gc_ref[...] * heads_to_lanes(out)


def select_kernel(dev_ref, pick_ref, qt_ref, kv_ref, gs_ref, cmp_ref, *refs):
    in_refs, out_ref = refs[:2 * SIDE], refs[2 * SIDE]
    q_scr, k_scr, gs_scr, cmp_scr, o_scr, in_scr, in_sem, sem, out_sem = refs[2 * SIDE + 1:]
    count = out_ref.shape[0]
    dev = dev_ref[0]
    z, x = dev // SIDE, dev % SIDE
    first = dev * count
    own_rows = k_scr.at[:, pl.ds(0, Q_BLOCK), :]
    early = [
        pltpu.make_async_copy(qt_ref, q_scr, sem.at[0]),
        pltpu.make_async_copy(kv_ref, own_rows, sem.at[1]),
    ]
    groups = count // TOGETHER
    group_rows = lambda g: pl.ds(g * TOGETHER, TOGETHER)
    arriving = [
        [pltpu.make_async_copy(ref.at[group_rows(g)], in_scr.at[k, group_rows(g)], in_sem.at[g])
         for k, ref in enumerate(in_refs)]
        for g in range(groups)
    ]
    late = [
        pltpu.make_async_copy(gs_ref, gs_scr, sem.at[2]),
        pltpu.make_async_copy(cmp_ref, cmp_scr, sem.at[3]),
    ]
    for copy in early + arriving[0] + late + sum(arriving[1:], []):
        copy.start()
    for copy in early:
        copy.wait()
    low = lax.broadcasted_iota(jnp.int32, (Q_BLOCK, LANES), 1) < HEAD_DIM
    row = lax.broadcasted_iota(jnp.int32, (2 * Q_BLOCK, Q_BLOCK), 0) % Q_BLOCK
    causal = lax.broadcasted_iota(jnp.int32, (2 * Q_BLOCK, Q_BLOCK), 1) <= row
    far_keys = FAR_PICKS * SEL_BLOCK
    pick_of = lax.broadcasted_iota(jnp.int32, (1, far_keys), 1) // SEL_BLOCK
    low_k = lax.broadcasted_iota(jnp.int32, (Q_BLOCK + far_keys, LANES), 1) < HEAD_DIM

    def body(group, carry):
        scored = []
        landed = in_scr.at[:, group_rows(group)]
        pltpu.make_async_copy(landed, landed, in_sem.at[group]).wait()
        for u in range(TOGETHER):
            block = group * TOGETHER + u
            for j in range(FAR_PICKS):
                span = pick_ref[j, first + block] // SPAN_BLOCKS
                a, b = (x - span % SIDE) % SIDE, (z - span // SIDE) % SIDE
                row0 = Q_BLOCK + j * SEL_BLOCK
                k_scr[block, row0:row0 + HALF, :] = in_scr[a, block, b]
                k_scr[block, row0 + HALF:row0 + SEL_BLOCK, :] = in_scr[SIDE + b, block, a]
        for u in range(TOGETHER):
            block = group * TOGETHER + u
            keys = k_scr[block]
            scored.append((block, keys, dot_nt(q_scr[:, block].reshape(2 * Q_BLOCK, LANES), keys)))
        weighed = []
        for block, keys, scores in scored:
            index = first + block
            bias = jnp.zeros((1, far_keys), F32)
            for j in range(FAR_PICKS):
                later = pick_ref[j, index] >= index * (Q_BLOCK // SEL_BLOCK)
                bias = jnp.where(pick_of == j, jnp.where(later, MASKED, 0.0), bias)
            own = jnp.where(causal, scores[:, :Q_BLOCK], MASKED)
            scores = jnp.concatenate([own, scores[:, Q_BLOCK:] + bias], axis=1)
            top = jnp.max(scores, axis=1, keepdims=True)
            weighed.append((block, keys, jnp.exp2(scores - top).astype(BF16)))

        @pl.when(group == 0)
        def _():
            for copy in late:
                copy.wait()

        for block, keys, probs in weighed:
            values = jnp.where(low_k, 1.0, keys.astype(F32)).astype(BF16)
            mixed = jnp.dot(probs, values, preferred_element_type=F32)
            out = mixed / pltpu.roll(mixed, HEAD_DIM, 1)
            joined = jnp.where(low, pltpu.roll(out[:Q_BLOCK], HEAD_DIM, 1), out[Q_BLOCK:])
            o_scr[block] = (cmp_scr[block] + gs_scr[block] * joined).astype(BF16)
            pltpu.make_async_copy(o_scr.at[block], out_ref.at[block], out_sem).start()
        return carry

    lax.fori_loop(0, count // TOGETHER, body, 0)
    pltpu.make_async_copy(o_scr, out_ref, out_sem).wait()


def whole(shape):
    return pl.BlockSpec(shape, lambda i, *_: (0,) * len(shape))


def per_device(
    tokens, norm_gain, query_weight, cmp_key_weight, cmp_value_weight, sel_key_weight, sel_value_weight,
    branch_weight, key_embed, key_inner, key_outer, value_embed, value_inner, value_outer, out_weight, chosen,
):
    tok_rows, width = tokens.shape
    owners = lax.axis_size("kv")
    dev = lax.axis_index("kv")
    tp = lax.axis_index("tp")
    span_queries = tok_rows // Q_BLOCK
    span_blocks = tok_rows // SEL_BLOCK
    cmp_blocks = tok_rows // CMP_BLOCK
    picks = chosen[0].T
    dev = dev.astype(jnp.int32).reshape(1)
    tp = tp.astype(jnp.int32).reshape(1)

    coarse, fine = rope_tables(owners * tok_rows)
    steps = tok_rows // TILE
    gates_t = branch_weight.transpose(0, 2, 1).reshape(-1, width)
    half_blocks = lambda *n: jax.ShapeDtypeStruct((*n, HALF, LANES), BF16)
    inputs = [
        tokens, norm_gain.reshape(-1, LANES), query_weight, sel_key_weight.T, sel_value_weight.T,
        cmp_key_weight.T, cmp_value_weight.T, gates_t, jnp.asarray(fine), jnp.asarray(coarse),
        key_embed[0], key_inner[0].T, key_outer[0], value_embed[0], value_inner[0].T, value_outer[0],
    ]
    outputs = [
        jax.ShapeDtypeStruct((2, tok_rows, LANES), BF16),
        jax.ShapeDtypeStruct((2, tok_rows, LANES), BF16),
        jax.ShapeDtypeStruct((span_blocks, SEL_BLOCK, LANES), BF16),
        jax.ShapeDtypeStruct((tok_rows, LANES), F32),
        jax.ShapeDtypeStruct((tok_rows, LANES), F32),
        half_blocks(span_blocks + cmp_blocks // HALF),
        half_blocks(span_blocks),
    ]
    local = [pltpu.VMEM(v.shape, v.dtype) for v in inputs]
    local[0] = pltpu.VMEM((steps, TILE, width), BF16)
    local[9] = pltpu.VMEM((steps, 2, LANES), F32)
    any_space = pl.BlockSpec(memory_space=pl.ANY)
    big = pltpu.CompilerParams(dimension_semantics=("arbitrary",), vmem_limit_bytes=67_043_328)
    qp, qt, kv, gate_cmp, gate_sel, top, bottom = pl.pallas_call(
        project_kernel,
        grid_spec=pltpu.PrefetchScalarGridSpec(
            num_scalar_prefetch=2,
            grid=(1,),
            in_specs=[any_space] * len(inputs),
            out_specs=[any_space] * len(outputs),
            scratch_shapes=[
                *local,
                *[pltpu.VMEM(v.shape, v.dtype) for v in outputs[:5]],
                pltpu.VMEM((cmp_blocks // HALF, HALF, LANES), BF16),
                pltpu.VMEM((width, 4 * LANES), BF16),
                pltpu.VMEM((TILE, 4 * LANES), F32),
                pltpu.VMEM((TILE, 1), F32),
                pltpu.VMEM((TILE, LANES), F32),
                pltpu.VMEM((cmp_blocks, CMP_BLOCK * HEAD_DIM), F32),
                pltpu.VMEM((cmp_blocks, CMP_BLOCK * HEAD_DIM), F32),
                pltpu.SemaphoreType.DMA((steps,)),
                pltpu.SemaphoreType.DMA((len(inputs) - 1,)),
                pltpu.SemaphoreType.DMA((len(outputs) + 1,)),
            ],
        ),
        out_shape=outputs,
        compiler_params=big,
        name="project",
    )(dev, tp, *inputs)
    def along(axis, k):
        pairs = []
        for d in range(owners):
            dz, dx = d // SIDE, d % SIDE
            pairs.append((d, (dz + k) % SIDE * SIDE + dx if axis == "z" else dz * SIDE + (dx + k) % SIDE))
        return pairs

    shift = lambda v, axis, k: v if k == 0 else lax.ppermute(v, "kv", along(axis, k))
    order = (1, 3, 2)
    tops = {0: top}
    bottoms = {0: bottom}
    for k in order:
        tops[k] = shift(top, "z", k)
    for k in order:
        bottoms[k] = shift(bottom, "x", k)
    column = pl.pallas_call(
        column_kernel,
        in_specs=[any_space] * SIDE,
        out_specs=any_space,
        scratch_shapes=[pltpu.SemaphoreType.DMA((SIDE,))],
        out_shape=half_blocks(SIDE * cmp_blocks // HALF),
        compiler_params=pltpu.CompilerParams(vmem_limit_bytes=67_043_328),
        name="column",
    )(*[tops[k] for k in range(SIDE)])
    columns = [shift(column, "x", k) for k in range(SIDE)]
    packed = pl.pallas_call(
        pack_kernel,
        grid_spec=pltpu.PrefetchScalarGridSpec(
            num_scalar_prefetch=1,
            grid=(1,),
            in_specs=[whole(picks.shape)] + [whole(top.shape)] * SIDE + [whole(bottom.shape)] * SIDE,
            out_specs=[any_space] * (2 * SIDE),
            scratch_shapes=[
                pltpu.VMEM((2 * SIDE, span_queries, SIDE, HALF, LANES), BF16),
                pltpu.VMEM((2 * SIDE, picks.shape[1]), jnp.int32),
                pltpu.SMEM((2 * SIDE, picks.shape[1]), jnp.int32),
                pltpu.SemaphoreType.DMA,
                pltpu.SemaphoreType.DMA((2 * SIDE,)),
            ],
        ),
        out_shape=[half_blocks(span_queries, SIDE)] * (2 * SIDE),
        compiler_params=big,
        name="pack",
    )(dev, picks, *[tops[k] for k in range(SIDE)], *[bottoms[k] for k in range(SIDE)])
    barrier = lax.optimization_barrier((*packed, *columns))
    packed, columns = barrier[:2 * SIDE], barrier[2 * SIDE:]
    incoming = {0: packed[0], SIDE: packed[SIDE]}
    for k in order:
        incoming[k] = shift(packed[k], "x", k)
        incoming[SIDE + k] = shift(packed[SIDE + k], "z", k)

    part = tok_rows // 4
    gated = pl.pallas_call(
        compress_kernel,
        grid_spec=pltpu.PrefetchScalarGridSpec(
            num_scalar_prefetch=1,
            grid=(4,),
            in_specs=[
                pl.BlockSpec((2, part, LANES), lambda i, *m: (0, i, 0)),
                pl.BlockSpec((part, LANES), lambda i, *m: (i, 0)),
                *[whole(column.shape)] * SIDE,
            ],
            out_specs=pl.BlockSpec((part, LANES), lambda i, *m: (i, 0)),
            scratch_shapes=[
                pltpu.VMEM((owners * cmp_blocks, LANES), BF16),
                pltpu.VMEM((HEAD_DIM, owners * cmp_blocks), BF16),
            ],
        ),
        out_shape=jax.ShapeDtypeStruct((tok_rows, LANES), F32),
        compiler_params=big,
        name="compress",
    )(dev, qp, gate_cmp, *columns)

    by_block = lambda v: v.reshape(span_queries, Q_BLOCK, LANES)
    far = FAR_PICKS * SEL_BLOCK
    mixed = pl.pallas_call(
        select_kernel,
        grid_spec=pltpu.PrefetchScalarGridSpec(
            num_scalar_prefetch=2,
            grid=(1,),
            in_specs=[any_space] * (4 + 2 * SIDE),
            out_specs=any_space,
            scratch_shapes=[
                pltpu.VMEM((2, span_queries, Q_BLOCK, LANES), BF16),
                pltpu.VMEM((span_queries, Q_BLOCK + far, LANES), BF16),
                pltpu.VMEM((span_queries, Q_BLOCK, LANES), F32),
                pltpu.VMEM((span_queries, Q_BLOCK, LANES), F32),
                pltpu.VMEM((span_queries, Q_BLOCK, LANES), BF16),
                pltpu.VMEM((2 * SIDE, span_queries, SIDE, HALF, LANES), BF16),
                pltpu.SemaphoreType.DMA((2 * SIDE,)),
                pltpu.SemaphoreType.DMA((4,)),
                pltpu.SemaphoreType.DMA,
            ],
        ),
        out_shape=jax.ShapeDtypeStruct((span_queries, Q_BLOCK, LANES), BF16),
        compiler_params=big,
        name="select",
    )(
        dev, picks, qt.reshape(2, span_queries, Q_BLOCK, LANES), by_block(kv), by_block(gate_sel),
        by_block(gated), *[incoming[k] for k in range(2 * SIDE)],
    )
    rows = lax.all_to_all(mixed.reshape(lax.axis_size("tp"), -1, LANES), "tp", 0, 0, tiled=True)
    weight = out_weight.reshape(rows.shape[0], LANES, out_weight.shape[1])
    return jnp.einsum("trc,tcd->rd", rows, weight, preferred_element_type=F32).astype(BF16)


def solution(mesh):
    placed = (
        P("kv", None),
        P(),
        P(None, "tp"),
        P(None, "tp"),
        P(None, "tp"),
        P(None, "tp"),
        P(None, "tp"),
        P(),
        P("tp", None, None),
        P("tp", None, None),
        P("tp", None, None),
        P("tp", None, None),
        P("tp", None, None),
        P("tp", None, None),
        P(),
        P("tp", None, None),
    )
    return jax.shard_map(
        per_device, mesh=mesh, in_specs=placed, out_specs=P(("kv", "tp"), None), check_vma=False
    )
```

```python
import functools

import jax
import jax.numpy as jnp
import numpy as np
from jax import lax
from jax.experimental import pallas as pl
from jax.experimental.pallas import tpu as pltpu
from jax.sharding import PartitionSpec as P

HEAD_DIM = 64
CMP_BLOCK = 32
SEL_BLOCK = 64
Q_BLOCK = 128
FAR_PICKS = 8
ROPE_BASE = 10000.0
NORM_EPS = 1e-06
MASKED = -1e30
LANES = 128
TILE = 256
SPAN_BLOCKS = 32
HALF = SEL_BLOCK // 2
SIDE = 4
LOG2E = 1.4426950408889634
TOGETHER = 4

F32 = jnp.float32
BF16 = jnp.bfloat16


def dot_nt(a, b):
    return lax.dot_general(a, b, (((1,), (1,)), ((), ())), preferred_element_type=F32)


def rope_tables(total):
    lane = np.arange(LANES)
    inverse = ROPE_BASE ** (-(lane % 32) / 32.0)
    sign = np.where(lane % 64 < 32, -1.0, 1.0)
    coarse = (np.arange(total // TILE) * TILE)[:, None] * inverse[None, :]
    fine = np.arange(TILE)[:, None] * inverse[None, :]
    pack = lambda a: np.stack([np.cos(a), np.sin(a) * sign[None, :]], axis=1).astype(np.float32)
    return pack(coarse), pack(fine).transpose(1, 0, 2)


def wanted_blocks(picks, dev, span_blocks):
    match = picks // span_blocks == dev
    return jnp.sum(jnp.where(match, picks % span_blocks, 0), axis=0, keepdims=True)


def scale_rows(ref, gain):
    return (ref[...].astype(F32) * gain).astype(BF16)


def gain_row(gain_scr):
    rows = gain_scr[...]
    return jnp.concatenate([rows[k:k + 1, :] for k in range(rows.shape[0])], axis=1)


def token_tiles(tok_ref, tok_scr, tok_sem):
    def tile_copy(t):
        return pltpu.make_async_copy(tok_ref.at[pl.ds(t * TILE, TILE), :], tok_scr.at[t], tok_sem.at[t])

    return tile_copy


def project_tiles(tile_copy, tok_scr, w_scr, raw_scr, inv_scr, epilogue, send):
    tiles = tok_scr.shape[0]

    def tile(step, carry):
        prev = jnp.maximum(step - 1, 0)
        now = jnp.minimum(step, tiles - 1)
        raw = raw_scr[...]
        inv = inv_scr[...]

        @pl.when(step < tiles)
        def _():
            tile_copy(now).wait()

        fresh = jnp.dot(tok_scr[now], w_scr[...], preferred_element_type=F32)
        squares = jnp.zeros((TILE, LANES), F32)
        for k in range(tok_scr.shape[2] // LANES):
            part = tok_scr[now, :, k * LANES:(k + 1) * LANES].astype(F32)
            squares = squares + part * part
        mean = jnp.sum(squares, axis=-1, keepdims=True) * (1.0 / tok_scr.shape[2])
        epilogue(prev, raw, inv)
        raw_scr[...] = fresh
        inv_scr[...] = lax.rsqrt(mean + NORM_EPS)

        @pl.when(step > 0)
        def _():
            for copy in send(prev):
                copy.start()

        return carry

    lax.fori_loop(0, tiles + 1, tile, 0)


def make_turn(coarse_scr, fine_scr, t):
    ch = coarse_scr[t, 0:1, :]
    sh = coarse_scr[t, 1:2, :]
    cl = fine_scr[0]
    sl = fine_scr[1]
    cosine = ch * cl - sh * sl
    sine = sh * cl + ch * sl
    lane = lax.broadcasted_iota(jnp.int32, (TILE, LANES), 1)
    first_half = (lane % HEAD_DIM) < 32

    def turn(v):
        swapped = jnp.where(first_half, pltpu.roll(v, LANES - 32, 1), pltpu.roll(v, 32, 1))
        return v * cosine + swapped * sine

    return turn


def wanted_blocks(picks, span, span_blocks):
    match = picks // span_blocks == span
    return jnp.sum(jnp.where(match, picks % span_blocks, 0), axis=0, keepdims=True)


def project_keys_kernel(dev_ref, *refs):
    n_in = 14
    tok_ref, coarse_ref, *rest = refs[:n_in]
    kv_ref, top_ref, bot_ref = refs[n_in:n_in + 3]
    tok_scr, coarse_scr, *local = refs[n_in + 3:2 * n_in + 3]
    gain_scr, sk_scr, sv_scr, ck_scr, cv_scr, fine_scr, ke_scr, ki_scr, ko_scr, ve_scr, vi_scr, vo_scr = local
    kv_scr, sum_scr, w_scr, raw_scr, inv_scr, c_scr, xk_scr, xv_scr, tok_sem, in_sem, out_sem = refs[2 * n_in + 3:]
    tiles = tok_scr.shape[0]
    span_blocks = kv_scr.shape[0]
    low = lax.broadcasted_iota(jnp.int32, (TILE, LANES), 1) < HEAD_DIM
    tile_copy = token_tiles(tok_ref, tok_scr, tok_sem)
    copies = [pltpu.make_async_copy(src, dst, in_sem.at[i]) for i, (src, dst) in enumerate(zip(rest, local))]
    copies.append(
        pltpu.make_async_copy(coarse_ref.at[pl.ds(dev_ref[0] * tiles, tiles)], coarse_scr, in_sem.at[len(local)])
    )
    for copy in copies[:5]:
        copy.start()
    tile_copy(0).start()
    for copy in copies[5:]:
        copy.start()
    for t in range(1, tiles):
        tile_copy(t).start()
    for copy in copies[:5]:
        copy.wait()
    gain = gain_row(gain_scr).astype(F32)
    w_scr[:, 0:LANES] = jnp.concatenate([scale_rows(sk_scr, gain), scale_rows(sv_scr, gain)], axis=0).T
    w_scr[:, LANES:2 * LANES] = jnp.concatenate([scale_rows(ck_scr, gain), scale_rows(cv_scr, gain)], axis=0).T
    for copy in copies[5:]:
        copy.wait()
    blocks = TILE // CMP_BLOCK
    low_b = lax.broadcasted_iota(jnp.int32, (blocks, LANES), 1) < HEAD_DIM
    per = TILE // SEL_BLOCK

    def epilogue(prev, raw, inv):
        kv = raw[:, 0:LANES] * inv
        kv = jnp.where(low, make_turn(coarse_scr, fine_scr, prev)(kv), kv).astype(BF16)
        kv_scr[pl.ds(prev * per, per)] = kv.reshape(per, SEL_BLOCK, LANES)
        c_scr[...] = (raw[:, LANES:2 * LANES] * inv).astype(BF16).astype(F32)
        embed = jnp.concatenate([ke_scr[...], ve_scr[...]], axis=1).astype(F32)
        part = pl.ds(pl.multiple_of(prev * blocks, blocks), blocks)
        for pair in range(CMP_BLOCK // 2):
            r = 2 * pair
            a = c_scr[pl.ds(r, blocks, stride=CMP_BLOCK), :] + embed[r:r + 1, :]
            b = c_scr[pl.ds(r + 1, blocks, stride=CMP_BLOCK), :] + embed[r + 1:r + 2, :]
            cols = slice(pair * LANES, (pair + 1) * LANES)
            xk_scr[part, cols] = jnp.where(low_b, a, pltpu.roll(b, HEAD_DIM, 1))
            xv_scr[part, cols] = jnp.where(low_b, pltpu.roll(a, HEAD_DIM, 1), b)

    def send(t):
        rows = pl.ds(t * per, per)
        pairs = (
            (kv_scr.at[rows], kv_ref.at[rows]),
            (kv_scr.at[rows, 0:HALF], top_ref.at[rows]),
            (kv_scr.at[rows, HALF:SEL_BLOCK], bot_ref.at[rows]),
        )
        return [pltpu.make_async_copy(src, dst, out_sem.at[i]) for i, (src, dst) in enumerate(pairs)]

    project_tiles(tile_copy, tok_scr, w_scr, raw_scr, inv_scr, epilogue, send)
    hidden_k = jax.nn.gelu(dot_nt(xk_scr[...].astype(BF16), ki_scr[...])).astype(BF16)
    hidden_v = jax.nn.gelu(dot_nt(xv_scr[...].astype(BF16), vi_scr[...])).astype(BF16)
    summary = jnp.concatenate(
        [
            jnp.dot(hidden_k, ko_scr[...], preferred_element_type=F32),
            jnp.dot(hidden_v, vo_scr[...], preferred_element_type=F32),
        ],
        axis=1,
    ).astype(BF16)
    sum_scr[...] = summary.reshape(sum_scr.shape)
    tail = pltpu.make_async_copy(sum_scr, top_ref.at[pl.ds(span_blocks, sum_scr.shape[0])], out_sem.at[3])
    tail.start()
    tail.wait()
    pairs = (
        (kv_scr, kv_ref),
        (kv_scr.at[:, 0:HALF], top_ref.at[pl.ds(0, span_blocks)]),
        (kv_scr.at[:, HALF:SEL_BLOCK], bot_ref),
    )
    for i, (src, dst) in enumerate(pairs):
        pltpu.make_async_copy(src, dst, out_sem.at[i]).wait()


def project_queries_kernel(dev_ref, tp_ref, *refs):
    n_in = 6
    tok_ref, coarse_ref, *rest = refs[:n_in]
    out_refs = refs[n_in:n_in + 4]
    tok_scr, coarse_scr, *local = refs[n_in + 4:2 * n_in + 4]
    gain_scr, wq_scr, bw_scr, fine_scr = local
    *out_scr, w_scr, raw_scr, inv_scr, tok_sem, in_sem, out_sem = refs[2 * n_in + 4:]
    qp_scr, qt_scr, gc_scr, gs_scr = out_scr
    tiles = tok_scr.shape[0]
    low = lax.broadcasted_iota(jnp.int32, (TILE, LANES), 1) < HEAD_DIM
    tile_copy = token_tiles(tok_ref, tok_scr, tok_sem)
    copies = [pltpu.make_async_copy(src, dst, in_sem.at[i]) for i, (src, dst) in enumerate(zip(rest, local))]
    copies.append(
        pltpu.make_async_copy(coarse_ref.at[pl.ds(dev_ref[0] * tiles, tiles)], coarse_scr, in_sem.at[len(local)])
    )
    for copy in copies:
        copy.start()
    for t in range(tiles):
        tile_copy(t).start()
    for copy in copies:
        copy.wait()
    gain = gain_row(gain_scr)
    gain_cols = jnp.broadcast_to(gain, (LANES, gain.shape[1])).T
    w_scr[:, 0:LANES] = (wq_scr[...].astype(F32) * gain_cols.astype(F32)).astype(BF16)
    bw = scale_rows(bw_scr, gain.astype(F32))
    pad = jnp.zeros((LANES - bw.shape[0], bw.shape[1]), BF16)
    w_scr[:, LANES:2 * LANES] = jnp.concatenate([bw, pad], axis=0).T

    def epilogue(prev, raw, inv):
        at = pl.ds(pl.multiple_of(prev * TILE, TILE), TILE)
        q = raw[:, 0:LANES] * (inv * (HEAD_DIM ** (-0.5) * LOG2E))
        turned = make_turn(coarse_scr, fine_scr, prev)(q)
        qp_scr[0, at, :] = jnp.where(low, q, 0.0).astype(BF16)
        qp_scr[1, at, :] = jnp.where(low, pltpu.roll(q, HEAD_DIM, 1), 0.0).astype(BF16)
        qt_scr[0, at, :] = jnp.where(low, turned, 0.0).astype(BF16)
        qt_scr[1, at, :] = jnp.where(low, pltpu.roll(turned, HEAD_DIM, 1), 0.0).astype(BF16)
        logits = pltpu.roll(raw[:, LANES:2 * LANES] * inv, LANES - tp_ref[0] * 2, 1)
        gates = 1.0 / (1.0 + jnp.exp(-logits))
        gc_scr[at, :] = jnp.where(low, gates[:, 0:1], gates[:, 1:2])
        gs_scr[at, :] = jnp.where(low, gates[:, 16:17], gates[:, 17:18])

    def send(t):
        at = pl.ds(pl.multiple_of(t * TILE, TILE), TILE)
        rows = lambda ref: ref.at[:, at, :] if len(ref.shape) == 3 else ref.at[at, :]
        return [
            pltpu.make_async_copy(rows(src), rows(dst), out_sem.at[i])
            for i, (src, dst) in enumerate(zip(out_scr, out_refs))
        ]

    project_tiles(tile_copy, tok_scr, w_scr, raw_scr, inv_scr, epilogue, send)
    for i, (src, dst) in enumerate(zip(out_scr, out_refs)):
        pltpu.make_async_copy(src, dst, out_sem.at[i]).wait()


def pack_kernel(dev_ref, pick_ref, *refs, side):
    sources, out_refs, rest = refs[:SIDE], refs[SIDE:2 * SIDE], refs[2 * SIDE:]
    if side == 0:
        column_ref, *rest = rest
    out_scr, want_vmem, want_smem, want_sem, column_sem, out_sem = rest
    dev = dev_ref[0]
    z, x = dev // SIDE, dev % SIDE
    picks = pick_ref[...]
    column_copies = []
    if side == 0:
        count = column_ref.shape[0] // SIDE
        for k, ref in enumerate(sources):
            source = ref.at[pl.ds(ref.shape[0] - count, count)]
            column_copies.append(
                pltpu.make_async_copy(source, column_ref.at[pl.ds(k * count, count)], column_sem.at[k])
            )
    for copy in column_copies:
        copy.start()
    for k in range(SIDE):
        span = (z - k) % SIDE * SIDE + x if side == 0 else z * SIDE + (x - k) % SIDE
        want_vmem[k:k + 1, :] = wanted_blocks(picks, span, SPAN_BLOCKS)
    fetch = pltpu.make_async_copy(want_vmem, want_smem, want_sem)
    fetch.start()
    fetch.wait()
    queries = out_scr.shape[1]
    for m in range(SIDE):
        dest = z * SIDE + (x + m) % SIDE if side == 0 else (z + m) % SIDE * SIDE + x

        def fill(n, carry):
            for k in range(SIDE):
                out_scr[m, n, k] = sources[k][want_smem[k, dest * queries + n]]
            return carry

        lax.fori_loop(0, queries, fill, 0)
        pltpu.make_async_copy(out_scr.at[m], out_refs[m], out_sem.at[m]).start()
    for copy in column_copies:
        copy.wait()
    for m in range(SIDE):
        pltpu.make_async_copy(out_scr.at[m], out_refs[m], out_sem.at[m]).wait()


def heads_to_lanes(out):
    rows = out.shape[1] // 2
    return jnp.concatenate([out[:, :rows], out[:, rows:]], axis=0).T


def compress_kernel(dev_ref, qp_ref, gc_ref, *refs):
    sum_refs, (out_ref, k_scr, v_scr) = refs[:SIDE], refs[SIDE:]
    count = k_scr.shape[0]
    blocks = count // SIDE // SIDE
    dev = dev_ref[0]
    z, x = dev // SIDE, dev % SIDE
    step = pl.program_id(0)

    @pl.when(step == 0)
    def _():
        lane = lax.broadcasted_iota(jnp.int32, (blocks, LANES), 1)
        for a in range(SIDE):
            for b in range(SIDE):
                slot = a * SIDE + b
                rows = slice(slot * blocks, (slot + 1) * blocks)
                span = (z - b) % SIDE * SIDE + (x - a) % SIDE
                pair = sum_refs[a][2 * b:2 * b + 2].reshape(blocks, LANES).astype(F32)
                hide = jnp.where(span <= dev, 0.0, MASKED)
                k_scr[rows, :] = jnp.where(
                    lane < HEAD_DIM, pair, jnp.where(lane == HEAD_DIM, hide, 0.0)
                ).astype(BF16)
                v_scr[:, rows] = pair.T[HEAD_DIM:, :].astype(BF16)

    size = qp_ref.shape[1]
    lane = lax.broadcasted_iota(jnp.int32, (2 * size, LANES), 1)
    col = lax.broadcasted_iota(jnp.int32, (1, 2 * size), 1) % size
    own = lax.broadcasted_iota(jnp.int32, (blocks, 2 * size), 0)
    limit = (step * size + col + 1) // CMP_BLOCK
    q = qp_ref[...].reshape(2 * size, LANES)
    q = jnp.where(lane == HEAD_DIM, 1.0, q.astype(F32)).astype(BF16)
    scores = dot_nt(k_scr[...], q)
    near = jnp.where(own < limit, scores[:blocks], MASKED)
    scores = jnp.concatenate([near, scores[blocks:]], axis=0)
    top = jnp.max(scores, axis=0, keepdims=True)
    probs = jnp.exp2(scores - top)
    total = jnp.sum(probs, axis=0, keepdims=True)
    out = jnp.dot(v_scr[...], probs.astype(BF16), preferred_element_type=F32)
    out = jnp.where((limit > 0) | (dev > 0), out / total, 0.0)
    out_ref[...] = gc_ref[...] * heads_to_lanes(out)


def select_kernel(dev_ref, pick_ref, qt_ref, kv_ref, gs_ref, cmp_ref, *refs):
    in_refs, out_ref = refs[:2 * SIDE], refs[2 * SIDE]
    q_scr, k_scr, gs_scr, cmp_scr, o_scr, in_scr, in_sem, sem, out_sem = refs[2 * SIDE + 1:]
    count = out_ref.shape[0]
    dev = dev_ref[0]
    z, x = dev // SIDE, dev % SIDE
    first = dev * count
    own_rows = k_scr.at[:, pl.ds(0, Q_BLOCK), :]
    early = [
        pltpu.make_async_copy(qt_ref, q_scr, sem.at[0]),
        pltpu.make_async_copy(kv_ref, own_rows, sem.at[1]),
    ]
    groups = count // TOGETHER
    group_rows = lambda g: pl.ds(g * TOGETHER, TOGETHER)
    arriving = [
        [pltpu.make_async_copy(ref.at[group_rows(g)], in_scr.at[k, group_rows(g)], in_sem.at[g])
         for k, ref in enumerate(in_refs)]
        for g in range(groups)
    ]
    late = [
        pltpu.make_async_copy(gs_ref, gs_scr, sem.at[2]),
        pltpu.make_async_copy(cmp_ref, cmp_scr, sem.at[3]),
    ]
    for copy in early + arriving[0] + late + sum(arriving[1:], []):
        copy.start()
    for copy in early:
        copy.wait()
    low = lax.broadcasted_iota(jnp.int32, (Q_BLOCK, LANES), 1) < HEAD_DIM
    row = lax.broadcasted_iota(jnp.int32, (2 * Q_BLOCK, Q_BLOCK), 0) % Q_BLOCK
    causal = lax.broadcasted_iota(jnp.int32, (2 * Q_BLOCK, Q_BLOCK), 1) <= row
    far_keys = FAR_PICKS * SEL_BLOCK
    pick_of = lax.broadcasted_iota(jnp.int32, (1, far_keys), 1) // SEL_BLOCK
    low_k = lax.broadcasted_iota(jnp.int32, (Q_BLOCK + far_keys, LANES), 1) < HEAD_DIM

    def body(group, carry):
        scored = []
        landed = in_scr.at[:, group_rows(group)]
        pltpu.make_async_copy(landed, landed, in_sem.at[group]).wait()
        for u in range(TOGETHER):
            block = group * TOGETHER + u
            for j in range(FAR_PICKS):
                span = pick_ref[j, first + block] // SPAN_BLOCKS
                a, b = (x - span % SIDE) % SIDE, (z - span // SIDE) % SIDE
                row0 = Q_BLOCK + j * SEL_BLOCK
                k_scr[block, row0:row0 + HALF, :] = in_scr[a, block, b]
                k_scr[block, row0 + HALF:row0 + SEL_BLOCK, :] = in_scr[SIDE + b, block, a]
        for u in range(TOGETHER):
            block = group * TOGETHER + u
            keys = k_scr[block]
            scored.append((block, keys, dot_nt(q_scr[:, block].reshape(2 * Q_BLOCK, LANES), keys)))
        weighed = []
        for block, keys, scores in scored:
            index = first + block
            bias = jnp.zeros((1, far_keys), F32)
            for j in range(FAR_PICKS):
                later = pick_ref[j, index] >= index * (Q_BLOCK // SEL_BLOCK)
                bias = jnp.where(pick_of == j, jnp.where(later, MASKED, 0.0), bias)
            own = jnp.where(causal, scores[:, :Q_BLOCK], MASKED)
            scores = jnp.concatenate([own, scores[:, Q_BLOCK:] + bias], axis=1)
            top = jnp.max(scores, axis=1, keepdims=True)
            weighed.append((block, keys, jnp.exp2(scores - top).astype(BF16)))

        @pl.when(group == 0)
        def _():
            for copy in late:
                copy.wait()

        for block, keys, probs in weighed:
            values = jnp.where(low_k, 1.0, keys.astype(F32)).astype(BF16)
            mixed = jnp.dot(probs, values, preferred_element_type=F32)
            out = mixed / pltpu.roll(mixed, HEAD_DIM, 1)
            joined = jnp.where(low, pltpu.roll(out[:Q_BLOCK], HEAD_DIM, 1), out[Q_BLOCK:])
            o_scr[block] = (cmp_scr[block] + gs_scr[block] * joined).astype(BF16)
            pltpu.make_async_copy(o_scr.at[block], out_ref.at[block], out_sem).start()
        return carry

    lax.fori_loop(0, count // TOGETHER, body, 0)
    pltpu.make_async_copy(o_scr, out_ref, out_sem).wait()


def whole(shape):
    return pl.BlockSpec(shape, lambda i, *_: (0,) * len(shape))


def per_device(
    tokens, norm_gain, query_weight, cmp_key_weight, cmp_value_weight, sel_key_weight, sel_value_weight,
    branch_weight, key_embed, key_inner, key_outer, value_embed, value_inner, value_outer, out_weight, chosen,
):
    tok_rows, width = tokens.shape
    owners = lax.axis_size("kv")
    dev = lax.axis_index("kv")
    tp = lax.axis_index("tp")
    span_queries = tok_rows // Q_BLOCK
    span_blocks = tok_rows // SEL_BLOCK
    cmp_blocks = tok_rows // CMP_BLOCK
    picks = chosen[0].T
    dev = dev.astype(jnp.int32).reshape(1)
    tp = tp.astype(jnp.int32).reshape(1)

    coarse, fine = rope_tables(owners * tok_rows)
    steps = tok_rows // TILE
    gates_t = branch_weight.transpose(0, 2, 1).reshape(-1, width)
    half_blocks = lambda *n: jax.ShapeDtypeStruct((*n, HALF, LANES), BF16)
    coarse, fine = jnp.asarray(coarse), jnp.asarray(fine)
    gain = norm_gain.reshape(-1, LANES)
    any_space = pl.BlockSpec(memory_space=pl.ANY)
    big = pltpu.CompilerParams(dimension_semantics=("arbitrary",), vmem_limit_bytes=67_043_328)

    def call(kernel, scalars, inputs, outputs, scratch, name):
        local = [pltpu.VMEM(v.shape, v.dtype) for v in inputs]
        local[0] = pltpu.VMEM((steps, TILE, width), BF16)
        local[1] = pltpu.VMEM((steps, 2, LANES), F32)
        return pl.pallas_call(
            kernel,
            grid_spec=pltpu.PrefetchScalarGridSpec(
                num_scalar_prefetch=len(scalars),
                grid=(1,),
                in_specs=[any_space] * len(inputs),
                out_specs=[any_space] * len(outputs),
                scratch_shapes=[
                    *local,
                    *scratch,
                    pltpu.SemaphoreType.DMA((steps,)),
                    pltpu.SemaphoreType.DMA((len(inputs) - 1,)),
                    pltpu.SemaphoreType.DMA((4,)),
                ],
            ),
            out_shape=outputs,
            compiler_params=big,
            name=name,
        )(*scalars, *inputs)

    matmul_scratch = [
        pltpu.VMEM((width, 2 * LANES), BF16),
        pltpu.VMEM((TILE, 2 * LANES), F32),
        pltpu.VMEM((TILE, 1), F32),
    ]
    kv_shape = jax.ShapeDtypeStruct((span_blocks, SEL_BLOCK, LANES), BF16)
    kv, top, bottom = call(
        project_keys_kernel,
        [dev],
        [
            tokens, coarse, gain, sel_key_weight.T, sel_value_weight.T, cmp_key_weight.T, cmp_value_weight.T, fine,
            key_embed[0], key_inner[0].T, key_outer[0], value_embed[0], value_inner[0].T, value_outer[0],
        ],
        [kv_shape, half_blocks(span_blocks + cmp_blocks // HALF), half_blocks(span_blocks)],
        [
            pltpu.VMEM(kv_shape.shape, BF16),
            pltpu.VMEM((cmp_blocks // HALF, HALF, LANES), BF16),
            *matmul_scratch,
            pltpu.VMEM((TILE, LANES), F32),
            pltpu.VMEM((cmp_blocks, CMP_BLOCK * HEAD_DIM), F32),
            pltpu.VMEM((cmp_blocks, CMP_BLOCK * HEAD_DIM), F32),
        ],
        "keys",
    )

    def along(axis, k):
        pairs = []
        for d in range(owners):
            dz, dx = d // SIDE, d % SIDE
            pairs.append((d, (dz + k) % SIDE * SIDE + dx if axis == "z" else dz * SIDE + (dx + k) % SIDE))
        return pairs

    shift = lambda v, axis, k: v if k == 0 else lax.ppermute(v, "kv", along(axis, k))
    order = (1, 3, 2)
    tops = {0: top}
    bottoms = {0: bottom}
    for k in order:
        tops[k] = shift(top, "z", k)
    for k in order:
        bottoms[k] = shift(bottom, "x", k)

    def pack(sources, side):
        column_out = [half_blocks(SIDE * cmp_blocks // HALF)] * (side == 0)
        return pl.pallas_call(
            functools.partial(pack_kernel, side=side),
            grid_spec=pltpu.PrefetchScalarGridSpec(
                num_scalar_prefetch=1,
                grid=(1,),
                in_specs=[whole(picks.shape)] + [whole(sources[0].shape)] * SIDE,
                out_specs=[any_space] * (SIDE + len(column_out)),
                scratch_shapes=[
                    pltpu.VMEM((SIDE, span_queries, SIDE, HALF, LANES), BF16),
                    pltpu.VMEM((SIDE, picks.shape[1]), jnp.int32),
                    pltpu.SMEM((SIDE, picks.shape[1]), jnp.int32),
                    pltpu.SemaphoreType.DMA,
                    pltpu.SemaphoreType.DMA((SIDE,)),
                    pltpu.SemaphoreType.DMA((SIDE,)),
                ],
            ),
            out_shape=[half_blocks(span_queries, SIDE)] * SIDE + column_out,
            compiler_params=big,
            name="pack",
        )(dev, picks, *[sources[k] for k in range(SIDE)])

    *packed_top, column = pack(tops, 0)
    columns = [shift(column, "x", k) for k in range(SIDE)]
    packed_bottom = pack(bottoms, 1)
    packed = [*packed_top, *packed_bottom]
    barrier = lax.optimization_barrier((*packed, *columns, tokens))
    packed, columns, tokens = barrier[:2 * SIDE], barrier[2 * SIDE:-1], barrier[-1]
    gates_shape = jax.ShapeDtypeStruct((tok_rows, LANES), F32)
    heads_shape = jax.ShapeDtypeStruct((2, tok_rows, LANES), BF16)
    query_out = [heads_shape, heads_shape, gates_shape, gates_shape]
    qp, qt, gate_cmp, gate_sel = call(
        project_queries_kernel,
        [dev, tp],
        [tokens, coarse, gain, query_weight, gates_t, fine],
        query_out,
        [*[pltpu.VMEM(v.shape, v.dtype) for v in query_out], *matmul_scratch],
        "queries",
    )
    incoming = {0: packed[0], SIDE: packed[SIDE]}
    for k in order:
        incoming[k] = shift(packed[k], "x", k)
        incoming[SIDE + k] = shift(packed[SIDE + k], "z", k)

    part = tok_rows // 4
    gated = pl.pallas_call(
        compress_kernel,
        grid_spec=pltpu.PrefetchScalarGridSpec(
            num_scalar_prefetch=1,
            grid=(4,),
            in_specs=[
                pl.BlockSpec((2, part, LANES), lambda i, *m: (0, i, 0)),
                pl.BlockSpec((part, LANES), lambda i, *m: (i, 0)),
                *[whole(column.shape)] * SIDE,
            ],
            out_specs=pl.BlockSpec((part, LANES), lambda i, *m: (i, 0)),
            scratch_shapes=[
                pltpu.VMEM((owners * cmp_blocks, LANES), BF16),
                pltpu.VMEM((HEAD_DIM, owners * cmp_blocks), BF16),
            ],
        ),
        out_shape=jax.ShapeDtypeStruct((tok_rows, LANES), F32),
        compiler_params=big,
        name="compress",
    )(dev, qp, gate_cmp, *columns)

    by_block = lambda v: v.reshape(span_queries, Q_BLOCK, LANES)
    far = FAR_PICKS * SEL_BLOCK
    mixed = pl.pallas_call(
        select_kernel,
        grid_spec=pltpu.PrefetchScalarGridSpec(
            num_scalar_prefetch=2,
            grid=(1,),
            in_specs=[any_space] * (4 + 2 * SIDE),
            out_specs=any_space,
            scratch_shapes=[
                pltpu.VMEM((2, span_queries, Q_BLOCK, LANES), BF16),
                pltpu.VMEM((span_queries, Q_BLOCK + far, LANES), BF16),
                pltpu.VMEM((span_queries, Q_BLOCK, LANES), F32),
                pltpu.VMEM((span_queries, Q_BLOCK, LANES), F32),
                pltpu.VMEM((span_queries, Q_BLOCK, LANES), BF16),
                pltpu.VMEM((2 * SIDE, span_queries, SIDE, HALF, LANES), BF16),
                pltpu.SemaphoreType.DMA((2 * SIDE,)),
                pltpu.SemaphoreType.DMA((4,)),
                pltpu.SemaphoreType.DMA,
            ],
        ),
        out_shape=jax.ShapeDtypeStruct((span_queries, Q_BLOCK, LANES), BF16),
        compiler_params=big,
        name="select",
    )(
        dev, picks, qt.reshape(2, span_queries, Q_BLOCK, LANES), by_block(kv), by_block(gate_sel),
        by_block(gated), *[incoming[k] for k in range(2 * SIDE)],
    )
    rows = lax.all_to_all(mixed.reshape(lax.axis_size("tp"), -1, LANES), "tp", 0, 0, tiled=True)
    weight = out_weight.reshape(rows.shape[0], LANES, out_weight.shape[1])
    return jnp.einsum("trc,tcd->rd", rows, weight, preferred_element_type=F32).astype(BF16)


def solution(mesh):
    placed = (
        P("kv", None),
        P(),
        P(None, "tp"),
        P(None, "tp"),
        P(None, "tp"),
        P(None, "tp"),
        P(None, "tp"),
        P(),
        P("tp", None, None),
        P("tp", None, None),
        P("tp", None, None),
        P("tp", None, None),
        P("tp", None, None),
        P("tp", None, None),
        P(),
        P("tp", None, None),
    )
    return jax.shard_map(
        per_device, mesh=mesh, in_specs=placed, out_specs=P(("kv", "tp"), None), check_vma=False
    )
```

```python
import functools

import jax
import jax.numpy as jnp
import numpy as np
from jax import lax
from jax.experimental import pallas as pl
from jax.experimental.pallas import tpu as pltpu
from jax.sharding import PartitionSpec as P


HEAD_DIM = 64
CMP_BLOCK = 32
SEL_BLOCK = 64
Q_BLOCK = 128
FAR_PICKS = 8
ROPE_BASE = 10000.0
NORM_EPS = 1e-06
MASKED = -1e30
LANES = 128
TILE = 512
SPAN_BLOCKS = 32
HALF = SEL_BLOCK // 2
SIDE = 4
SENDS = ("z1", "z3", "x1", "x3", "z2", "x2")
SPAN_SHIFT = 5
SIDE_SHIFT = 2
LOG2E = 1.4426950408889634
TOGETHER = 8

F32 = jnp.float32
BF16 = jnp.bfloat16


def dot_nt(a, b):
    return lax.dot_general(a, b, (((1,), (1,)), ((), ())), preferred_element_type=F32)


def rope_tables(total):
    lane = np.arange(LANES)
    inverse = ROPE_BASE ** (-(lane % 32) / 32.0)
    sign = np.where(lane % 64 < 32, -1.0, 1.0)
    coarse = (np.arange(total // TILE) * TILE)[:, None] * inverse[None, :]
    fine = np.arange(TILE)[:, None] * inverse[None, :]
    pack = lambda a: np.stack([np.cos(a), np.sin(a) * sign[None, :]], axis=1).astype(np.float32)
    return pack(coarse), pack(fine).transpose(1, 0, 2)


def wanted_blocks(picks, dev, span_blocks):
    match = picks // span_blocks == dev
    return jnp.sum(jnp.where(match, picks % span_blocks, 0), axis=0, keepdims=True)


def scale_rows(ref, gain):
    return (ref[...].astype(F32) * gain).astype(BF16)


def gain_row(gain_scr):
    rows = gain_scr[...]
    return jnp.concatenate([rows[k:k + 1, :] for k in range(rows.shape[0])], axis=1)


def rows_at(t, size):
    return pl.ds(t * size if isinstance(t, int) else pl.multiple_of(t * size, size), size)


def token_tiles(tok_ref, tok_scr, tok_sem):
    def tile_copy(t):
        return pltpu.make_async_copy(tok_ref.at[pl.ds(t * TILE, TILE), :], tok_scr.at[t], tok_sem.at[t])

    return tile_copy


def project_tiles(tile_copy, tok_scr, w_scr, raw_scr, inv_scr, epilogue, send):
    tiles = tok_scr.shape[0]

    def tile(step, carry):
        prev = jnp.maximum(step - 1, 0)
        now = step
        raw = raw_scr[...]
        inv = inv_scr[...]
        tile_copy(now).wait()
        fresh = jnp.dot(tok_scr[now], w_scr[...], preferred_element_type=F32)
        squares = jnp.zeros((TILE, LANES), F32)
        for k in range(tok_scr.shape[2] // LANES):
            part = tok_scr[now, :, k * LANES:(k + 1) * LANES].astype(F32)
            squares = squares + part * part
        mean = jnp.sum(squares, axis=-1, keepdims=True) * (1.0 / tok_scr.shape[2])
        epilogue(prev, raw, inv)
        raw_scr[...] = fresh
        inv_scr[...] = lax.rsqrt(mean + NORM_EPS)

        @pl.when(step > 0)
        def _():
            for copy in send(prev):
                copy.start()

        return carry

    lax.fori_loop(0, tiles, tile, 0)
    epilogue(tiles - 1, raw_scr[...], inv_scr[...])
    for copy in send(tiles - 1):
        copy.start()


def make_turn(coarse_scr, fine_scr, t):
    ch = coarse_scr[t, 0:1, :]
    sh = coarse_scr[t, 1:2, :]
    cl = fine_scr[0]
    sl = fine_scr[1]
    cosine = ch * cl - sh * sl
    sine = sh * cl + ch * sl
    lane = lax.broadcasted_iota(jnp.int32, (TILE, LANES), 1)
    first_half = (lane % HEAD_DIM) < 32

    def turn(v):
        swapped = jnp.where(first_half, pltpu.roll(v, LANES - 32, 1), pltpu.roll(v, 32, 1))
        return v * cosine + swapped * sine

    return turn


def wanted_blocks(picks, span, span_blocks):
    match = picks // span_blocks == span
    return jnp.sum(jnp.where(match, picks % span_blocks, 0), axis=0, keepdims=True)


def project_keys_kernel(dev_ref, *refs):
    n_in = 15
    tok_ref, coarse_ref, *rest = refs[:n_in]
    kv_ref, top_ref, bot_ref, want_ref = refs[n_in:n_in + 4]
    tok_scr, coarse_scr, *local = refs[n_in + 4:2 * n_in + 4]
    gain_scr, sk_scr, sv_scr, ck_scr, cv_scr, fine_scr, ke_scr, ki_scr, ko_scr, ve_scr, vi_scr, vo_scr, pick_scr = local
    (
        kv_scr, sum_scr, w_scr, raw_scr, inv_scr, c_scr, xk_scr, xv_scr, want_scr, tok_sem, in_sem, out_sem,
    ) = refs[2 * n_in + 4:]
    tiles = tok_scr.shape[0]
    span_blocks = kv_scr.shape[0]
    low = lax.broadcasted_iota(jnp.int32, (TILE, LANES), 1) < HEAD_DIM
    tile_copy = token_tiles(tok_ref, tok_scr, tok_sem)
    copies = [pltpu.make_async_copy(src, dst, in_sem.at[i]) for i, (src, dst) in enumerate(zip(rest, local))]
    copies.append(
        pltpu.make_async_copy(coarse_ref.at[pl.ds(dev_ref[0] * tiles, tiles)], coarse_scr, in_sem.at[len(local)])
    )
    for copy in copies[:5]:
        copy.start()
    tile_copy(0).start()
    for copy in copies[5:]:
        copy.start()
    for t in range(1, tiles):
        tile_copy(t).start()
    for copy in copies[:5]:
        copy.wait()
    gain = gain_row(gain_scr).astype(F32)
    w_scr[:, 0:LANES] = jnp.concatenate([scale_rows(sk_scr, gain), scale_rows(sv_scr, gain)], axis=0).T
    w_scr[:, LANES:2 * LANES] = jnp.concatenate([scale_rows(ck_scr, gain), scale_rows(cv_scr, gain)], axis=0).T
    for copy in copies[5:]:
        copy.wait()
    z, x = dev_ref[0] // SIDE, dev_ref[0] % SIDE
    picks = pick_scr[...]
    for k in range(SIDE):
        want_scr[k:k + 1, :] = wanted_blocks(picks, (z - k) % SIDE * SIDE + x, SPAN_BLOCKS)
        want_scr[SIDE + k:SIDE + k + 1, :] = wanted_blocks(picks, z * SIDE + (x - k) % SIDE, SPAN_BLOCKS)
    want_copy = pltpu.make_async_copy(want_scr, want_ref, out_sem.at[4])
    want_copy.start()
    blocks = TILE // CMP_BLOCK
    low_b = lax.broadcasted_iota(jnp.int32, (blocks, LANES), 1) < HEAD_DIM
    per = TILE // SEL_BLOCK

    def epilogue(prev, raw, inv):
        kv = raw[:, 0:LANES] * inv
        kv = jnp.where(low, make_turn(coarse_scr, fine_scr, prev)(kv), kv).astype(BF16)
        kv_scr[pl.ds(prev * per, per)] = kv.reshape(per, SEL_BLOCK, LANES)
        c_scr[...] = (raw[:, LANES:2 * LANES] * inv).astype(BF16).astype(F32)
        embed = jnp.concatenate([ke_scr[...], ve_scr[...]], axis=1).astype(F32)
        part = rows_at(prev, blocks)
        for pair in range(CMP_BLOCK // 2):
            r = 2 * pair
            a = c_scr[pl.ds(r, blocks, stride=CMP_BLOCK), :] + embed[r:r + 1, :]
            b = c_scr[pl.ds(r + 1, blocks, stride=CMP_BLOCK), :] + embed[r + 1:r + 2, :]
            cols = slice(pair * LANES, (pair + 1) * LANES)
            xk_scr[part, cols] = jnp.where(low_b, a, pltpu.roll(b, HEAD_DIM, 1))
            xv_scr[part, cols] = jnp.where(low_b, pltpu.roll(a, HEAD_DIM, 1), b)

    def send(t):
        rows = pl.ds(t * per, per)
        pairs = (
            (kv_scr.at[rows], kv_ref.at[rows]),
            (kv_scr.at[rows, 0:HALF], top_ref.at[rows]),
            (kv_scr.at[rows, HALF:SEL_BLOCK], bot_ref.at[rows]),
        )
        return [pltpu.make_async_copy(src, dst, out_sem.at[i]) for i, (src, dst) in enumerate(pairs)]

    project_tiles(tile_copy, tok_scr, w_scr, raw_scr, inv_scr, epilogue, send)
    hidden_k = jax.nn.gelu(dot_nt(xk_scr[...].astype(BF16), ki_scr[...])).astype(BF16)
    hidden_v = jax.nn.gelu(dot_nt(xv_scr[...].astype(BF16), vi_scr[...])).astype(BF16)
    summary = jnp.concatenate(
        [
            jnp.dot(hidden_k, ko_scr[...], preferred_element_type=F32),
            jnp.dot(hidden_v, vo_scr[...], preferred_element_type=F32),
        ],
        axis=1,
    ).astype(BF16)
    sum_scr[...] = summary.reshape(sum_scr.shape)
    tail = pltpu.make_async_copy(sum_scr, top_ref.at[pl.ds(span_blocks, sum_scr.shape[0])], out_sem.at[3])
    tail.start()
    tail.wait()
    want_copy.wait()
    pairs = (
        (kv_scr, kv_ref),
        (kv_scr.at[:, 0:HALF], top_ref.at[pl.ds(0, span_blocks)]),
        (kv_scr.at[:, HALF:SEL_BLOCK], bot_ref),
    )
    for i, (src, dst) in enumerate(pairs):
        pltpu.make_async_copy(src, dst, out_sem.at[i]).wait()


def project_queries_kernel(dev_ref, tp_ref, *refs):
    n_in = 6
    tok_ref, coarse_ref, *rest = refs[:n_in]
    out_refs = refs[n_in:n_in + 4]
    tok_scr, coarse_scr, *local = refs[n_in + 4:2 * n_in + 4]
    gain_scr, wq_scr, bw_scr, fine_scr = local
    *out_scr, w_scr, raw_scr, inv_scr, tok_sem, in_sem, out_sem = refs[2 * n_in + 4:]
    qp_scr, qt_scr, gc_scr, gs_scr = out_scr
    tiles = tok_scr.shape[0]
    low = lax.broadcasted_iota(jnp.int32, (TILE, LANES), 1) < HEAD_DIM
    tile_copy = token_tiles(tok_ref, tok_scr, tok_sem)
    copies = [pltpu.make_async_copy(src, dst, in_sem.at[i]) for i, (src, dst) in enumerate(zip(rest, local))]
    copies.append(
        pltpu.make_async_copy(coarse_ref.at[pl.ds(dev_ref[0] * tiles, tiles)], coarse_scr, in_sem.at[len(local)])
    )
    for copy in copies:
        copy.start()
    for t in range(tiles):
        tile_copy(t).start()
    for copy in copies:
        copy.wait()
    gain = gain_row(gain_scr)
    gain_cols = jnp.broadcast_to(gain, (LANES, gain.shape[1])).T
    w_scr[:, 0:LANES] = (wq_scr[...].astype(F32) * gain_cols.astype(F32)).astype(BF16)
    bw = scale_rows(bw_scr, gain.astype(F32))
    pad = jnp.zeros((LANES - bw.shape[0], bw.shape[1]), BF16)
    w_scr[:, LANES:2 * LANES] = jnp.concatenate([bw, pad], axis=0).T

    def epilogue(prev, raw, inv):
        at = rows_at(prev, TILE)
        q = raw[:, 0:LANES] * (inv * (HEAD_DIM ** (-0.5) * LOG2E))
        turned = make_turn(coarse_scr, fine_scr, prev)(q)
        qp_scr[0, at, :] = jnp.where(low, q, 0.0).astype(BF16)
        qp_scr[1, at, :] = jnp.where(low, pltpu.roll(q, HEAD_DIM, 1), 0.0).astype(BF16)
        qt_scr[0, at, :] = jnp.where(low, turned, 0.0).astype(BF16)
        qt_scr[1, at, :] = jnp.where(low, pltpu.roll(turned, HEAD_DIM, 1), 0.0).astype(BF16)
        logits = pltpu.roll(raw[:, LANES:2 * LANES] * inv, LANES - tp_ref[0] * 2, 1)
        gates = 1.0 / (1.0 + jnp.exp(-logits))
        gc_scr[at, :] = jnp.where(low, gates[:, 0:1], gates[:, 1:2])
        gs_scr[at, :] = jnp.where(low, gates[:, 16:17], gates[:, 17:18])

    def send(t):
        at = rows_at(t, TILE)
        rows = lambda ref: ref.at[:, at, :] if len(ref.shape) == 3 else ref.at[at, :]
        return [
            pltpu.make_async_copy(rows(src), rows(dst), out_sem.at[i])
            for i, (src, dst) in enumerate(zip(out_scr, out_refs))
        ]

    project_tiles(tile_copy, tok_scr, w_scr, raw_scr, inv_scr, epilogue, send)
    for i, (src, dst) in enumerate(zip(out_scr, out_refs)):
        pltpu.make_async_copy(src, dst, out_sem.at[i]).wait()


def pack_kernel(dev_ref, want_ref, *refs, side):
    sources, out_refs, rest = refs[:SIDE], refs[SIDE:2 * SIDE], refs[2 * SIDE:]
    if side == 0:
        column_ref, *rest = rest
    out_scr, column_sem, out_sem = rest
    dev = dev_ref[0]
    z, x = dev // SIDE, dev % SIDE
    column_copies = []
    if side == 0:
        count = column_ref.shape[0] // SIDE
        for k, ref in enumerate(sources):
            source = ref.at[pl.ds(ref.shape[0] - count, count)]
            column_copies.append(
                pltpu.make_async_copy(source, column_ref.at[pl.ds(k * count, count)], column_sem.at[k])
            )
    for copy in column_copies:
        copy.start()
    queries = out_scr.shape[1]
    for m in range(SIDE):
        dest = z * SIDE + (x + m) % SIDE if side == 0 else (z + m) % SIDE * SIDE + x

        def fill(n, carry):
            for k in range(SIDE):
                out_scr[m, n, k] = sources[k][want_ref[side * SIDE + k, dest * queries + n]]
            return carry

        lax.fori_loop(0, queries, fill, 0)
        pltpu.make_async_copy(out_scr.at[m], out_refs[m], out_sem.at[m]).start()
    for copy in column_copies:
        copy.wait()
    for m in range(SIDE):
        pltpu.make_async_copy(out_scr.at[m], out_refs[m], out_sem.at[m]).wait()


def heads_to_lanes(out):
    rows = out.shape[1] // 2
    return jnp.concatenate([out[:, :rows], out[:, rows:]], axis=0).T


def compress_kernel(dev_ref, qp_ref, gc_ref, *refs):
    sum_refs, (out_ref, k_scr, v_scr) = refs[:SIDE], refs[SIDE:]
    count = k_scr.shape[0]
    blocks = count // SIDE // SIDE
    dev = dev_ref[0]
    z, x = dev // SIDE, dev % SIDE
    step = pl.program_id(0)

    @pl.when(step == 0)
    def _():
        lane = lax.broadcasted_iota(jnp.int32, (blocks, LANES), 1)
        for a in range(SIDE):
            for b in range(SIDE):
                slot = a * SIDE + b
                rows = slice(slot * blocks, (slot + 1) * blocks)
                span = (z - b) % SIDE * SIDE + (x - a) % SIDE
                pair = sum_refs[a][2 * b:2 * b + 2].reshape(blocks, LANES).astype(F32)
                hide = jnp.where(span <= dev, 0.0, MASKED)
                k_scr[rows, :] = jnp.where(
                    lane < HEAD_DIM, pair, jnp.where(lane == HEAD_DIM, hide, 0.0)
                ).astype(BF16)
                v_scr[:, rows] = pair.T[HEAD_DIM:, :].astype(BF16)

    size = qp_ref.shape[1]
    lane = lax.broadcasted_iota(jnp.int32, (2 * size, LANES), 1)
    col = lax.broadcasted_iota(jnp.int32, (1, 2 * size), 1) % size
    own = lax.broadcasted_iota(jnp.int32, (blocks, 2 * size), 0)
    limit = (step * size + col + 1) // CMP_BLOCK
    q = qp_ref[...].reshape(2 * size, LANES)
    q = jnp.where(lane == HEAD_DIM, 1.0, q.astype(F32)).astype(BF16)
    scores = dot_nt(k_scr[...], q)
    near = jnp.where(own < limit, scores[:blocks], MASKED)
    scores = jnp.concatenate([near, scores[blocks:]], axis=0)
    top = jnp.max(scores, axis=0, keepdims=True)
    probs = jnp.exp2(scores - top)
    total = jnp.sum(probs, axis=0, keepdims=True)
    out = jnp.dot(v_scr[...], probs.astype(BF16), preferred_element_type=F32)
    out = jnp.where((limit > 0) | (dev > 0), out / total, 0.0)
    out_ref[...] = gc_ref[...] * heads_to_lanes(out)


def select_kernel(dev_ref, pick_ref, qt_ref, kv_ref, gs_ref, cmp_ref, *refs):
    in_refs, out_ref = refs[:2 * SIDE], refs[2 * SIDE]
    q_scr, k_scr, gs_scr, cmp_scr, o_scr, in_scr, in_sem, q_sem, own_sem, sem, out_sem = refs[2 * SIDE + 1:]
    count = out_ref.shape[0]
    dev = dev_ref[0]
    z, x = dev // SIDE, dev % SIDE
    first = dev * count
    groups = count // TOGETHER
    group_rows = lambda g: pl.ds(g * TOGETHER, TOGETHER)
    own_rows = lambda g: k_scr.at[group_rows(g), pl.ds(0, Q_BLOCK), :]

    def query_copy(g):
        return pltpu.make_async_copy(qt_ref.at[:, group_rows(g)], q_scr.at[:, group_rows(g)], q_sem.at[g])

    def own_copy(g):
        return pltpu.make_async_copy(kv_ref.at[group_rows(g)], own_rows(g), own_sem.at[g])

    arriving = [
        [pltpu.make_async_copy(ref.at[group_rows(g)], in_scr.at[k, group_rows(g)], in_sem.at[g])
         for k, ref in enumerate(in_refs)]
        + [query_copy(g), own_copy(g)]
        for g in range(groups)
    ]
    late = [
        pltpu.make_async_copy(gs_ref, gs_scr, sem.at[0]),
        pltpu.make_async_copy(cmp_ref, cmp_scr, sem.at[1]),
    ]
    for copy in arriving[0] + late + sum(arriving[1:], []):
        copy.start()
    low = lax.broadcasted_iota(jnp.int32, (Q_BLOCK, LANES), 1) < HEAD_DIM
    row = lax.broadcasted_iota(jnp.int32, (2 * Q_BLOCK, Q_BLOCK), 0) % Q_BLOCK
    causal = lax.broadcasted_iota(jnp.int32, (2 * Q_BLOCK, Q_BLOCK), 1) <= row
    far_keys = FAR_PICKS * SEL_BLOCK
    pick_of = lax.broadcasted_iota(jnp.int32, (1, far_keys), 1) // SEL_BLOCK
    low_k = lax.broadcasted_iota(jnp.int32, (Q_BLOCK + far_keys, LANES), 1) < HEAD_DIM

    def body(group, carry):
        scored = []
        landed = in_scr.at[:, group_rows(group)]
        pltpu.make_async_copy(landed, landed, in_sem.at[group]).wait()
        query_copy(group).wait()
        own_copy(group).wait()
        for u in range(TOGETHER):
            block = group * TOGETHER + u
            for j in range(FAR_PICKS):
                span = lax.shift_right_logical(pick_ref[j, first + block], SPAN_SHIFT)
                a = (x - span) & (SIDE - 1)
                b = (z - lax.shift_right_logical(span, SIDE_SHIFT)) & (SIDE - 1)
                row0 = Q_BLOCK + j * SEL_BLOCK
                k_scr[block, row0:row0 + HALF, :] = in_scr[a, block, b]
                k_scr[block, row0 + HALF:row0 + SEL_BLOCK, :] = in_scr[SIDE + b, block, a]
        for u in range(TOGETHER):
            block = group * TOGETHER + u
            keys = k_scr[block]
            scored.append((block, keys, dot_nt(q_scr[:, block].reshape(2 * Q_BLOCK, LANES), keys)))
        weighed = []
        for block, keys, scores in scored:
            index = first + block
            bias = jnp.zeros((1, far_keys), F32)
            for j in range(FAR_PICKS):
                later = pick_ref[j, index] >= index * (Q_BLOCK // SEL_BLOCK)
                bias = jnp.where(pick_of == j, jnp.where(later, MASKED, 0.0), bias)
            own = jnp.where(causal, scores[:, :Q_BLOCK], MASKED)
            scores = jnp.concatenate([own, scores[:, Q_BLOCK:] + bias], axis=1)
            top = jnp.max(scores, axis=1, keepdims=True)
            weighed.append((block, keys, jnp.exp2(scores - top).astype(BF16)))

        @pl.when(group == 0)
        def _():
            for copy in late:
                copy.wait()

        for block, keys, probs in weighed:
            values = jnp.where(low_k, 1.0, keys.astype(F32)).astype(BF16)
            mixed = jnp.dot(probs, values, preferred_element_type=F32)
            out = mixed / pltpu.roll(mixed, HEAD_DIM, 1)
            joined = jnp.where(low, pltpu.roll(out[:Q_BLOCK], HEAD_DIM, 1), out[Q_BLOCK:])
            o_scr[block] = (cmp_scr[block] + gs_scr[block] * joined).astype(BF16)
            pltpu.make_async_copy(o_scr.at[block], out_ref.at[block], out_sem).start()
        return carry

    lax.fori_loop(0, count // TOGETHER, body, 0)
    pltpu.make_async_copy(o_scr, out_ref, out_sem).wait()


def whole(shape):
    return pl.BlockSpec(shape, lambda i, *_: (0,) * len(shape))


def per_device(
    tokens, norm_gain, query_weight, cmp_key_weight, cmp_value_weight, sel_key_weight, sel_value_weight,
    branch_weight, key_embed, key_inner, key_outer, value_embed, value_inner, value_outer, out_weight, chosen,
):
    tok_rows, width = tokens.shape
    owners = lax.axis_size("kv")
    dev = lax.axis_index("kv")
    tp = lax.axis_index("tp")
    span_queries = tok_rows // Q_BLOCK
    span_blocks = tok_rows // SEL_BLOCK
    cmp_blocks = tok_rows // CMP_BLOCK
    picks = chosen[0].T
    dev = dev.astype(jnp.int32).reshape(1)
    tp = tp.astype(jnp.int32).reshape(1)

    coarse, fine = rope_tables(owners * tok_rows)
    steps = tok_rows // TILE
    gates_t = branch_weight.transpose(0, 2, 1).reshape(-1, width)
    half_blocks = lambda *n: jax.ShapeDtypeStruct((*n, HALF, LANES), BF16)
    coarse, fine = jnp.asarray(coarse), jnp.asarray(fine)
    gain = norm_gain.reshape(-1, LANES)
    any_space = pl.BlockSpec(memory_space=pl.ANY)
    big = pltpu.CompilerParams(dimension_semantics=("arbitrary",), vmem_limit_bytes=67_043_328)

    def call(kernel, scalars, inputs, outputs, scratch):
        local = [pltpu.VMEM(v.shape, v.dtype) for v in inputs]
        local[0] = pltpu.VMEM((steps, TILE, width), BF16)
        local[1] = pltpu.VMEM((steps, 2, LANES), F32)
        return pl.pallas_call(
            kernel,
            grid_spec=pltpu.PrefetchScalarGridSpec(
                num_scalar_prefetch=len(scalars),
                grid=(1,),
                in_specs=[any_space] * len(inputs),
                out_specs=[any_space] * len(outputs),
                scratch_shapes=[
                    *local,
                    *scratch,
                    pltpu.SemaphoreType.DMA((steps,)),
                    pltpu.SemaphoreType.DMA((len(inputs) - 1,)),
                    pltpu.SemaphoreType.DMA((5,)),
                ],
            ),
            out_shape=outputs,
            compiler_params=big,
        )(*scalars, *inputs)

    matmul_scratch = [
        pltpu.VMEM((width, 2 * LANES), BF16),
        pltpu.VMEM((TILE, 2 * LANES), F32),
        pltpu.VMEM((TILE, 1), F32),
    ]
    kv_shape = jax.ShapeDtypeStruct((span_blocks, SEL_BLOCK, LANES), BF16)
    want_shape = jax.ShapeDtypeStruct((2 * SIDE, picks.shape[1]), jnp.int32)
    kv, top, bottom, wanted = call(
        project_keys_kernel,
        [dev],
        [
            tokens, coarse, gain, sel_key_weight.T, sel_value_weight.T, cmp_key_weight.T, cmp_value_weight.T, fine,
            key_embed[0], key_inner[0].T, key_outer[0], value_embed[0], value_inner[0].T, value_outer[0],
            picks,
        ],
        [kv_shape, half_blocks(span_blocks + cmp_blocks // HALF), half_blocks(span_blocks), want_shape],
        [
            pltpu.VMEM(kv_shape.shape, BF16),
            pltpu.VMEM((cmp_blocks // HALF, HALF, LANES), BF16),
            *matmul_scratch,
            pltpu.VMEM((TILE, LANES), F32),
            pltpu.VMEM((cmp_blocks, CMP_BLOCK * HEAD_DIM), F32),
            pltpu.VMEM((cmp_blocks, CMP_BLOCK * HEAD_DIM), F32),
            pltpu.VMEM(want_shape.shape, jnp.int32),
        ],
    )

    def along(axis, k):
        pairs = []
        for d in range(owners):
            dz, dx = d // SIDE, d % SIDE
            pairs.append((d, (dz + k) % SIDE * SIDE + dx if axis == "z" else dz * SIDE + (dx + k) % SIDE))
        return pairs

    shift = lambda v, axis, k: v if k == 0 else lax.ppermute(v, "kv", along(axis, k))
    order = (1, 3, 2)
    tops = {0: top}
    bottoms = {0: bottom}
    for k in order:
        tops[k] = shift(top, "z", k)
    for k in order:
        bottoms[k] = shift(bottom, "x", k)

    def pack(sources, side):
        column_out = [half_blocks(SIDE * cmp_blocks // HALF)] * (side == 0)
        return pl.pallas_call(
            functools.partial(pack_kernel, side=side),
            grid_spec=pltpu.PrefetchScalarGridSpec(
                num_scalar_prefetch=2,
                grid=(1,),
                in_specs=[whole(sources[0].shape)] * SIDE,
                out_specs=[any_space] * (SIDE + len(column_out)),
                scratch_shapes=[
                    pltpu.VMEM((SIDE, span_queries, SIDE, HALF, LANES), BF16),
                    pltpu.SemaphoreType.DMA((SIDE,)),
                    pltpu.SemaphoreType.DMA((SIDE,)),
                ],
            ),
            out_shape=[half_blocks(span_queries, SIDE)] * SIDE + column_out,
            compiler_params=big,
            name="pack",
        )(dev, wanted, *[sources[k] for k in range(SIDE)])

    *packed_top, column = pack(tops, 0)
    columns = [shift(column, "x", k) for k in range(SIDE)]
    packed_bottom = pack(bottoms, 1)
    packed = [*packed_top, *packed_bottom]
    barrier = lax.optimization_barrier((*packed, tokens))
    packed, tokens = barrier[:-1], barrier[-1]
    gates_shape = jax.ShapeDtypeStruct((tok_rows, LANES), F32)
    heads_shape = jax.ShapeDtypeStruct((2, tok_rows, LANES), BF16)
    query_out = [heads_shape, heads_shape, gates_shape, gates_shape]
    qp, qt, gate_cmp, gate_sel = call(
        project_queries_kernel,
        [dev, tp],
        [tokens, coarse, gain, query_weight, gates_t, fine],
        query_out,
        [*[pltpu.VMEM(v.shape, v.dtype) for v in query_out], *matmul_scratch],
    )
    incoming = {0: packed[0], SIDE: packed[SIDE]}
    for name in SENDS:
        k = int(name[1])
        slot = k if name[0] == "x" else SIDE + k
        incoming[slot] = shift(packed[slot], name[0], k)

    part = tok_rows // 4
    gated = pl.pallas_call(
        compress_kernel,
        grid_spec=pltpu.PrefetchScalarGridSpec(
            num_scalar_prefetch=1,
            grid=(4,),
            in_specs=[
                pl.BlockSpec((2, part, LANES), lambda i, *m: (0, i, 0)),
                pl.BlockSpec((part, LANES), lambda i, *m: (i, 0)),
                *[whole(column.shape)] * SIDE,
            ],
            out_specs=pl.BlockSpec((part, LANES), lambda i, *m: (i, 0)),
            scratch_shapes=[
                pltpu.VMEM((owners * cmp_blocks, LANES), BF16),
                pltpu.VMEM((HEAD_DIM, owners * cmp_blocks), BF16),
            ],
        ),
        out_shape=jax.ShapeDtypeStruct((tok_rows, LANES), F32),
        compiler_params=big,
        name="compress",
    )(dev, qp, gate_cmp, *columns)

    by_block = lambda v: v.reshape(span_queries, Q_BLOCK, LANES)
    far = FAR_PICKS * SEL_BLOCK
    mixed = pl.pallas_call(
        select_kernel,
        grid_spec=pltpu.PrefetchScalarGridSpec(
            num_scalar_prefetch=2,
            grid=(1,),
            in_specs=[any_space] * (4 + 2 * SIDE),
            out_specs=any_space,
            scratch_shapes=[
                pltpu.VMEM((2, span_queries, Q_BLOCK, LANES), BF16),
                pltpu.VMEM((span_queries, Q_BLOCK + far, LANES), BF16),
                pltpu.VMEM((span_queries, Q_BLOCK, LANES), F32),
                pltpu.VMEM((span_queries, Q_BLOCK, LANES), F32),
                pltpu.VMEM((span_queries, Q_BLOCK, LANES), BF16),
                pltpu.VMEM((2 * SIDE, span_queries, SIDE, HALF, LANES), BF16),
                pltpu.SemaphoreType.DMA((span_queries // TOGETHER,)),
                pltpu.SemaphoreType.DMA((span_queries // TOGETHER,)),
                pltpu.SemaphoreType.DMA((span_queries // TOGETHER,)),
                pltpu.SemaphoreType.DMA((2,)),
                pltpu.SemaphoreType.DMA,
            ],
        ),
        out_shape=jax.ShapeDtypeStruct((span_queries, Q_BLOCK, LANES), BF16),
        compiler_params=pltpu.CompilerParams(
            dimension_semantics=("arbitrary",), vmem_limit_bytes=62_000_000
        ),
        name="select",
    )(
        dev, picks, qt.reshape(2, span_queries, Q_BLOCK, LANES), by_block(kv), by_block(gate_sel),
        by_block(gated), *[incoming[k] for k in range(2 * SIDE)],
    )
    rows = lax.all_to_all(mixed.reshape(lax.axis_size("tp"), -1, LANES), "tp", 0, 0, tiled=True)
    weight = out_weight.reshape(rows.shape[0], LANES, out_weight.shape[1])
    return jnp.einsum("trc,tcd->rd", rows, weight, preferred_element_type=F32).astype(BF16)


def solution(mesh):
    placed = (
        P("kv", None),
        P(),
        P(None, "tp"),
        P(None, "tp"),
        P(None, "tp"),
        P(None, "tp"),
        P(None, "tp"),
        P(),
        P("tp", None, None),
        P("tp", None, None),
        P("tp", None, None),
        P("tp", None, None),
        P("tp", None, None),
        P("tp", None, None),
        P(),
        P("tp", None, None),
    )

    return jax.shard_map(per_device, mesh=mesh, in_specs=placed, out_specs=P(("kv", "tp"), None), check_vma=False)
```
